256 devices in a mesh: ra: 32 (over z, x), cb: 4 (over y), dp: 2 (over core).
Axes of the slice: x: 4, y: 4, z: 8, core: 2. Of those that a mesh axis runs over, the one named last changes fastest.
Arguments:
- tokens: bfloat16 [256, 4096], P('dp', 'ra'), may hold values from -24 to 24
- first_gain: float32 [4096], P('ra'), may hold values from 0.1 to 1.9
- first_gate: float32 [4096, 11264], P('ra', 'cb'), may hold values from -0.1875 to 0.1875
- first_gate_scale: float32 [11264], P('cb'), may hold values from 0.5 to 2
- first_up: float32 [4096, 11264], P('ra', 'cb'), may hold values from -0.1875 to 0.1875
- first_up_scale: float32 [11264], P('cb'), may hold values from 0.5 to 2
- first_down: float32 [11264, 4096], P('cb', 'ra'), may hold values from -0.0546875 to 0.0546875
- first_down_scale: float32 [4096], P('ra'), may hold values from 0.5 to 2
- second_gain: float32 [4096], P('ra'), may hold values from 0.1 to 1.9
- second_gate: float32 [4096, 11264], P('ra', 'cb'), may hold values from -0.1875 to 0.1875
- second_gate_scale: float32 [11264], P('cb'), may hold values from 0.5 to 2
- second_up: float32 [4096, 11264], P('ra', 'cb'), may hold values from -0.1875 to 0.1875
- second_up_scale: float32 [11264], P('cb'), may hold values from 0.5 to 2
- second_down: float32 [11264, 4096], P('cb', 'ra'), may hold values from -0.0546875 to 0.0546875
- second_down_scale: float32 [4096], P('ra'), may hold values from 0.5 to 2
Outputs:
- mixed: float32 [256, 4096], P('dp', 'ra')
The draws below stay inside these ranges and needn't reach their ends.
All inputs are finite; a program needn't handle non-finite values.
Results may differ from the reference program's by a relative error of at most 0.0083.
Values may be sent and summed in bfloat16 or wider, within the bound.
No kernel may reach another device: no remote copies, remote signals or barrier semaphores. Data moves between devices by JAX's collectives and lax.ppermute only.
A program may use at most 64 MiB of HBM per device.

```python
import math
import jax
import jax.numpy as jnp
from jax import lax

D = 4096
FF = 11264
TOKENS = 256


def draw_tokens(key, part):
    first, second, third = jax.random.split(key, 3)
    values = jax.random.normal(first, (TOKENS, D), jnp.float32)
    blocks = jnp.exp(jax.random.uniform(second, (32,), jnp.float32, -1.2, 1.2))
    columns = jnp.repeat(blocks, D // 32)
    rows = jnp.exp(jax.random.uniform(third, (TOKENS, 1), jnp.float32, -0.7, 0.7))
    values = values * rows
    return jnp.clip(values * columns, -24.0, 24.0).astype(jnp.bfloat16)


def strengthened(drawn, rng, source, target, blocks, factor):
    owner, partner = [(jnp.arange(drawn.shape[dim]) // (drawn.shape[dim] // blocks)).reshape([-1 if axis == dim else 1 for axis in range(drawn.ndim)]) for dim in (source, target)]
    chosen = jax.random.permutation(rng, blocks)[partner]
    strong = (owner == chosen) | (owner == (partner + blocks // 2) % blocks)
    return jnp.where(strong, factor * drawn, drawn)


def block_scale(own_key, shape, cuts, least, top_value):
    def one(position, shards_of):
        draws = jax.random.uniform(jax.random.fold_in(jax.random.fold_in(own_key, 6), position), (shards_of,), jnp.float32, least / len(cuts), top_value / len(cuts))
        return jnp.repeat(jnp.exp(draws), shape[position] // shards_of).reshape((-1,) + (1,) * (len(shape) - position - 1))

    level = one(*cuts[0])
    for cut in cuts[1:]:
        level = level * one(*cut)
    return level


def scatter_about(own_key, shape, spread, most, cuts=(), held_as=jnp.bfloat16):
    result = jax.random.normal(own_key, shape, jnp.float32) * spread
    if len(cuts) > 0:
        result = block_scale(own_key, shape, cuts, -0.22, 0.18) * result
    return jnp.clip(result, min=-most, max=most).astype(held_as)


def noise_with(stream_key, extent, deviation, most, shards, heavy, kind=jnp.bfloat16):
    drawn = deviation * jax.random.normal(stream_key, extent, jnp.float32)
    if shards:
        drawn = drawn * block_scale(stream_key, extent, shards, -0.22, 0.18)
    return jnp.clip(strengthened(drawn, jax.random.fold_in(stream_key, 3), *heavy), -most, most).astype(kind)


def setup_inputs(seed: int = 0) -> dict:
    seeds = jax.random.split(jax.random.key(seed), 16)
    tokens = draw_tokens(jax.random.fold_in(seeds[15], 71), 0)
    first_gain = jnp.clip(1.0 + 0.18 * jax.random.normal(seeds[1], (D,), jnp.float32), 0.1, 1.9)
    first_gate = noise_with(seeds[2], (D, FF), D ** -0.5, 0.1875, ((0, 32), (1, 4)), (0, 1, 32, 2.75), jnp.float32)
    first_gate_scale = jnp.clip(jnp.exp(math.log(2.0) - 1.3862944 * jax.random.uniform(seeds[3], (FF,), jnp.float32) ** block_scale(seeds[3], (FF,), ((0, 4),), -0.2, 0.2)), 0.5, 2.0)
    first_up = noise_with(seeds[4], (D, FF), D ** -0.5, 0.1875, ((0, 32), (1, 4)), (0, 1, 32, 2.75), jnp.float32)
    first_up_scale = jnp.clip(jnp.exp(math.log(2.0) - 1.3862944 * jax.random.uniform(seeds[5], (FF,), jnp.float32) ** block_scale(seeds[5], (FF,), ((0, 4),), -0.2, 0.2)), 0.5, 2.0)
    first_down = scatter_about(seeds[6], (FF, D), FF ** -0.5, 0.0546875, ((0, 4), (1, 32)), jnp.float32)
    first_down_scale = jnp.clip(jnp.exp(math.log(2.0) - 1.3862944 * jax.random.uniform(seeds[7], (D,), jnp.float32) ** block_scale(seeds[7], (D,), ((0, 32),), -0.2, 0.2)), 0.5, 2.0)
    second_gain = jnp.clip(1.0 + 0.18 * jax.random.normal(seeds[8], (D,), jnp.float32), 0.1, 1.9)
    second_gate = noise_with(seeds[9], (D, FF), D ** -0.5, 0.1875, ((0, 32), (1, 4)), (0, 1, 32, 2.75), jnp.float32)
    second_gate_scale = jnp.clip(jnp.exp(math.log(2.0) - 1.3862944 * jax.random.uniform(seeds[10], (FF,), jnp.float32) ** block_scale(seeds[10], (FF,), ((0, 4),), -0.2, 0.2)), 0.5, 2.0)
    second_up = noise_with(seeds[11], (D, FF), D ** -0.5, 0.1875, ((0, 32), (1, 4)), (0, 1, 32, 2.75), jnp.float32)
    second_up_scale = jnp.clip(jnp.exp(math.log(2.0) - 1.3862944 * jax.random.uniform(seeds[12], (FF,), jnp.float32) ** block_scale(seeds[12], (FF,), ((0, 4),), -0.2, 0.2)), 0.5, 2.0)
    second_down = scatter_about(seeds[13], (FF, D), FF ** -0.5, 0.0546875, ((0, 4), (1, 32)), jnp.float32)
    second_down_scale = jnp.clip(jnp.exp(math.log(2.0) - 1.3862944 * jax.random.uniform(seeds[14], (D,), jnp.float32) ** block_scale(seeds[14], (D,), ((0, 32),), -0.2, 0.2)), 0.5, 2.0)
    return dict(tokens=tokens, first_gain=first_gain, first_gate=first_gate, first_gate_scale=first_gate_scale, first_up=first_up, first_up_scale=first_up_scale, first_down=first_down, first_down_scale=first_down_scale, second_gain=second_gain, second_gate=second_gate, second_gate_scale=second_gate_scale, second_up=second_up, second_up_scale=second_up_scale, second_down=second_down, second_down_scale=second_down_scale)


def half_step(stream, gain, gate_w, gate_scale, up_w, up_scale, down_w, down_scale):
    inverse = lax.rsqrt(lax.optimization_barrier(jnp.mean(stream * stream, axis=1, keepdims=True)) + 1e-06)
    scaled = (stream * gain).astype(jnp.bfloat16)
    gate = jnp.dot(scaled, gate_w.astype(jnp.bfloat16), preferred_element_type=jnp.float32) * inverse * gate_scale
    up = jnp.dot(scaled, up_w.astype(jnp.bfloat16), preferred_element_type=jnp.float32) * inverse * up_scale
    hidden = (jax.nn.silu(gate) * up).astype(jnp.bfloat16)
    branch = jnp.dot(hidden, down_w.astype(jnp.bfloat16), preferred_element_type=jnp.float32) * down_scale
    return 0.5 * stream + 0.5 * branch

def reference(tokens, first_gain, first_gate, first_gate_scale, first_up, first_up_scale, first_down, first_down_scale, second_gain, second_gate, second_gate_scale, second_up, second_up_scale, second_down, second_down_scale):
    stream = tokens.astype(jnp.float32)
    stream = half_step(stream, first_gain, first_gate, first_gate_scale, first_up, first_up_scale, first_down, first_down_scale)
    stream = half_step(stream, second_gain, second_gate, second_gate_scale, second_up, second_up_scale, second_down, second_down_scale)
    return stream
```

```python
import jax
import jax.numpy as jnp
from jax import lax
from jax.sharding import Mesh
from jax.sharding import PartitionSpec as P

BF = jnp.bfloat16
F32 = jnp.float32
XY = ("x", "y")


def swap(v, axis, size):
    return lax.all_to_all(v, axis, 0, 0, tiled=True)


def to_all(v, axis):
    n = lax.axis_size(axis)
    return lax.all_to_all(jnp.broadcast_to(v[None], (n, *v.shape)), axis, 0, 0, tiled=True)


def other_core(v):
    return lax.ppermute(v, "c", [(0, 1), (1, 0)])


def half_of(v, c, dim):
    first = lax.index_in_dim(v, 0, dim, keepdims=False)
    second = lax.index_in_dim(v, 1, dim, keepdims=False)
    return jnp.where(c == 0, first, second)


def pack_up(gate, up, gain, c):
    nx = lax.axis_size("x")
    rows, cols = gate.shape
    parts = []
    for w in (gate, up):
        scaled = (w * gain[:, None]).astype(BF)
        parts.append(half_of(scaled.reshape(rows, nx, 2, cols // nx // 2), c, 2))
    packed = jnp.concatenate(parts, axis=2)
    return packed.transpose(1, 0, 2)


def pack_down(down, c):
    nx = lax.axis_size("x")
    rows, cols = down.shape
    return half_of(down.astype(BF).reshape(nx, 2, rows // nx // 2, cols), c, 1)


def reshard(packed):
    own = lax.all_to_all(packed, "x", 0, 0, tiled=True)
    return own, other_core(own)


def scales_of(scale, x, c):
    size = scale.shape[0] // lax.axis_size("x") // 2
    base = x * 2 * size
    return (
        lax.dynamic_slice_in_dim(scale, base + c * size, size, 0),
        lax.dynamic_slice_in_dim(scale, base + (1 - c) * size, size, 0),
    )


def hidden_part(stream, ups, gate_scale, up_scale, x, c, width):
    nz = lax.axis_size("z")
    tokens = stream.shape[1]
    rows = tokens // nz
    flat = stream.transpose(1, 0, 2).reshape(tokens, -1)
    squares = jnp.sum(flat * flat, axis=1, keepdims=True)
    high = squares.astype(BF)
    low = (squares - high.astype(F32)).astype(BF)
    lanes = jnp.concatenate([jnp.broadcast_to(high, (tokens, 64)), jnp.broadcast_to(low, (tokens, 64))], axis=1)
    flat_bf = flat.astype(BF)
    sums = [
        jnp.dot(flat_bf, w.reshape(-1, w.shape[-1]), preferred_element_type=F32).astype(BF)
        for w in ups
    ]
    payload = jnp.concatenate([*sums, lanes], axis=1)
    got = lax.all_to_all(payload.reshape(nz, rows, -1), "z", 0, 0, tiled=True)
    total = jnp.sum(got.astype(F32), axis=0)
    half = sums[0].shape[1] // 2
    mean = jnp.sum(total[:, 4 * half :], axis=1, keepdims=True) / 64.0 / width
    inverse = lax.rsqrt(mean + 1e-06)
    gate_scales = scales_of(gate_scale, x, c)
    up_scales = scales_of(up_scale, x, c)
    hidden = []
    for k in range(2):
        gate = total[:, 2 * k * half : (2 * k + 1) * half] * inverse * gate_scales[k]
        up = total[:, (2 * k + 1) * half : (2 * k + 2) * half] * inverse * up_scales[k]
        hidden.append((jax.nn.silu(gate) * up).astype(BF))
    hidden = jnp.concatenate(hidden, axis=1)
    return to_all(hidden, "z").reshape(tokens, -1)


def down_part(hidden, downs):
    half = hidden.shape[1] // 2
    own = jnp.einsum("tf,xfd->xtd", hidden[:, :half], downs[0], preferred_element_type=F32)
    other = jnp.einsum("tf,xfd->xtd", hidden[:, half:], downs[1], preferred_element_type=F32)
    return (own + other).astype(BF)


def local(
    tokens,
    first_gain,
    first_gate,
    first_gate_scale,
    first_up,
    first_up_scale,
    first_down,
    first_down_scale,
    second_gain,
    second_gate,
    second_gate_scale,
    second_up,
    second_up_scale,
    second_down,
    second_down_scale,
):
    x = lax.axis_index("x")
    y = lax.axis_index("y")
    c = lax.axis_index("c")
    nx, ny, nz = lax.axis_size("x"), lax.axis_size("y"), lax.axis_size("z")
    n_tok, n_col = tokens.shape
    width = n_col * nx * nz
    rows = n_tok // ny

    first_ups = reshard(pack_up(first_gate, first_up, first_gain, c))
    stream = to_all(tokens, "x").astype(F32)
    first_downs = reshard(pack_down(first_down, c))
    second_ups = reshard(pack_up(second_gate, second_up, second_gain, c))
    second_downs = reshard(pack_down(second_down, c))

    hidden = hidden_part(stream, first_ups, first_gate_scale, first_up_scale, x, c, width)
    part = down_part(hidden, first_downs)
    got = lax.all_to_all(part.reshape(nx * ny, rows, n_col), XY, 0, 0, tiled=True)
    branch = jnp.sum(got.astype(F32), axis=0) * first_down_scale
    mine = lax.dynamic_slice_in_dim(tokens, y * rows, rows, 0).astype(F32)
    mine = 0.5 * mine + 0.5 * branch
    stream = to_all(mine, XY).reshape(nx, n_tok, n_col)

    hidden = hidden_part(stream, second_ups, second_gate_scale, second_up_scale, x, c, width)
    part = down_part(hidden, second_downs)
    spread = jnp.broadcast_to(part[:, None], (nx, ny, n_tok, n_col)).reshape(nx * ny, n_tok, n_col)
    got = lax.all_to_all(spread, XY, 0, 0, tiled=True)
    branch = jnp.sum(got.astype(F32), axis=0) * second_down_scale
    mine = lax.dynamic_index_in_dim(stream, x, 0, keepdims=False)
    return 0.5 * mine + 0.5 * branch


def solution(mesh):
    torus = Mesh(
        mesh.devices.reshape(8, 4, mesh.shape["cb"], mesh.shape["dp"]), ("z", "x", "y", "c")
    )
    ra = ("z", "x")
    wide, tall = P(ra, "y"), P("y", ra)
    half = (P(ra), wide, P("y"), wide, P("y"), tall, P(ra))
    in_specs = (P("c", ra), *half, *half)
    return jax.shard_map(
        local, mesh=torus, in_specs=in_specs, out_specs=P("c", ra), check_vma=False
    )
```

```python
import jax
import jax.numpy as jnp
from jax import lax
from jax.experimental import pallas as pl
from jax.experimental.pallas import tpu as pltpu
from jax.sharding import Mesh
from jax.sharding import PartitionSpec as P

BF = jnp.bfloat16
F32 = jnp.float32
XY = ("x", "y")
NX, NY, NZ = 4, 4, 8
N = 128
HALF = 352
PAD = 384
WIDE = 2 * PAD
CHUNK = 2 * HALF
WIDTH = 4096

SMEM = pl.BlockSpec(memory_space=pltpu.SMEM)
VMEM = pl.BlockSpec(memory_space=pltpu.VMEM)


def shape(*dims, dtype=BF):
    return jax.ShapeDtypeStruct(dims, dtype)


def call(body, outs, n_in, scratch=(), name=None):
    many = isinstance(outs, (list, tuple))
    return pl.pallas_call(
        body,
        out_shape=outs,
        in_specs=[SMEM] + [VMEM] * n_in,
        out_specs=[VMEM] * len(outs) if many else VMEM,
        scratch_shapes=list(scratch),
        name=name,
    )


def high_low(v):
    high = v.astype(BF).astype(F32)
    return high, (v - high).astype(BF).astype(F32)


def padded_chunk(ref, i):
    part = ref[:, i * HALF : (i + 1) * HALF]
    return jnp.concatenate([part, jnp.zeros((N, PAD - HALF), F32)], axis=1)


def with_columns(tile, first, second):
    lane = lax.broadcasted_iota(jnp.int32, tile.shape, 1)
    at = HALF - (PAD - N)
    return jnp.where(lane == at, first, jnp.where(lane == at + 1, second, tile))


def pack_first_body(at, gate, up, tokens, gain, p0, p1, p2, p3, other, chunks):
    x, c = at[0], at[2]
    for i in range(2 * NX):
        chunks[i, :, :PAD] = padded_chunk(gate, i).astype(BF)
        chunks[i, :, PAD:] = padded_chunk(up, i).astype(BF)
    stream = tokens[...].astype(F32)
    scaled = (stream * gain[...]).astype(BF)
    high, low = high_low(jnp.sum(stream * stream, axis=1, keepdims=True))
    for k, out in enumerate((p0, p1, p2, p3)):
        index = 2 * lax.rem(x + k, NX) + c
        out[:, :WIDE] = chunks[index]
        out[:, WIDE:] = scaled
        tile = chunks[index, :, PAD - N : PAD].astype(F32)
        out[:, PAD - N : PAD] = with_columns(tile, high, low).astype(BF)
    other[...] = chunks[2 * x + 1 - c]


def pack_second_body(at, gate, up, p0, p1, p2, p3, chunks):
    x = at[0]
    for i in range(2 * NX):
        chunks[i, :, :PAD] = padded_chunk(gate, i).astype(BF)
        chunks[i, :, PAD:] = padded_chunk(up, i).astype(BF)
    for k, out in enumerate((p0, p1, p2, p3)):
        index = 2 * lax.rem(x + k, NX)
        out[:, :WIDE] = chunks[index]
        out[:, WIDE:] = chunks[index + 1]


def pack_down_body(at, down, gain, p0, p1, p2, p3):
    x = at[0]
    value = gain[...]
    high = value.astype(BF).astype(F32)
    rest = value - high
    middle = rest.astype(BF).astype(F32)
    low = rest - middle
    row = lax.broadcasted_iota(jnp.int32, (PAD - HALF, N), 0)
    tail = jnp.where(row == 0, high, jnp.where(row == 1, middle, jnp.where(row == 2, low, 0.0)))
    tail = tail.astype(BF)
    for k, out in enumerate((p0, p1, p2, p3)):
        base = lax.rem(x + k, NX) * CHUNK
        for h in range(2):
            start = pl.multiple_of(base + h * HALF, 32)
            out[h * PAD : h * PAD + HALF, :] = down[pl.ds(start, HALF), :].astype(BF)
            out[h * PAD + HALF : (h + 1) * PAD, :] = tail


def store_payload(out, slot, sums, high, low):
    tile = with_columns(sums[:, PAD - N : PAD], high, low)
    sums = jnp.concatenate([sums[:, : PAD - N], tile, sums[:, PAD:]], axis=1)
    out[:, slot] = sums.astype(BF).reshape(NZ, N // NZ, WIDE)


def dot(a, b):
    return jnp.dot(a, b, preferred_element_type=F32)


def enter_first_body(at, r0, r1, r2, r3, q0, s1, s2, s3, out):
    c = at[2]
    mine = (r0, r1, r2, r3)
    theirs = (q0, s1, s2, s3)
    scaled = jnp.concatenate([r[:, WIDE:] for r in mine], axis=1)
    squares = jnp.zeros((N, N), F32)
    for r in mine:
        squares = squares + r[:, PAD - N : PAD].astype(F32)
    lane = lax.broadcasted_iota(jnp.int32, (N, N), 1)
    at_lane = HALF - (PAD - N)
    keep = (lane == at_lane) | (lane == at_lane + 1)
    squares = jnp.sum(jnp.where(keep, squares, 0.0), axis=1, keepdims=True)
    high, low = high_low(squares)
    for slot, group in ((c, mine), (1 - c, theirs)):
        weights = jnp.concatenate([r[:, :WIDE] for r in group], axis=0)
        store_payload(out, slot, dot(scaled, weights), high, low)


def enter_second_body(at, stream, d0, d1, d2, d3, w0, w1, w2, w3, out):
    x = at[0]
    scaled = []
    squares = jnp.zeros((N, 1), F32)
    for k, d in enumerate((d0, d1, d2, d3)):
        index = lax.rem(x + NX - k, NX)
        s = stream[pl.ds(index * NY, NY)].reshape(N, N)
        squares = squares + jnp.sum(s * s, axis=1, keepdims=True)
        tail = d[HALF:PAD, :].astype(F32)
        gain = tail[0:1] + tail[1:2] + tail[2:3]
        scaled.append((s * gain).astype(BF))
    scaled = jnp.concatenate(scaled, axis=1)
    high, low = high_low(squares)
    for slot in range(2):
        cols = slice(slot * WIDE, (slot + 1) * WIDE)
        weights = jnp.concatenate([w[:, cols] for w in (w0, w1, w2, w3)], axis=0)
        store_payload(out, slot, dot(scaled, weights), high, low)


def hidden_body(at, got, scales, out):
    rows = N // NZ
    tile = jnp.zeros((rows, N), F32)
    for z in range(NZ):
        tile = tile + got[z, 0, :, PAD - N : PAD].astype(F32)
    lane = lax.broadcasted_iota(jnp.int32, (rows, N), 1)
    at_lane = HALF - (PAD - N)
    keep = (lane == at_lane) | (lane == at_lane + 1)
    total = jnp.sum(jnp.where(keep, tile, 0.0), axis=1, keepdims=True)
    inverse = lax.rsqrt(total / WIDTH + 1e-06)
    for h in range(2):
        sums = got[0, h].astype(F32)
        for z in range(1, NZ):
            sums = sums + got[z, h].astype(F32)
        scaled = sums * inverse * scales[h : h + 1, :]
        gate = scaled[:, :PAD]
        hidden = gate / (1.0 + jnp.exp(-gate)) * scaled[:, PAD:]
        hidden = hidden.astype(BF)
        for z in range(NZ):
            out[z, h] = hidden


def down_sums(hidden, pieces):
    wide = jnp.concatenate([hidden[:, h].reshape(N, PAD) for h in range(2)], axis=1)
    return [dot(wide, d[...]).astype(BF) for d in pieces]


def leave_first_body(at, hidden, d0, d1, d2, d3, out):
    x = at[0]
    for k, part in enumerate(down_sums(hidden, (d0, d1, d2, d3))):
        index = lax.rem(x + NX - k, NX)
        out[pl.ds(index * NY, NY)] = part.reshape(NY, N // NY, N)


def leave_second_body(at, hidden, d0, d1, d2, d3, out):
    x = at[0]
    for k, part in enumerate(down_sums(hidden, (d0, d1, d2, d3))):
        index = lax.rem(x + NX - k, NX)
        for y in range(NY):
            out[index * NY + y] = part


def stream_body(at, got, tokens, scale, out):
    y = at[1]
    rows = N // NY
    branch = jnp.sum(got[...].astype(F32), axis=0) * scale[...]
    old = tokens[pl.ds(pl.multiple_of(y * rows, rows), rows), :].astype(F32)
    new = 0.5 * old + 0.5 * branch
    out[...] = jnp.broadcast_to(new[None], out.shape)


def final_body(at, got, stream, scale, out):
    x = at[0]
    branch = jnp.sum(got[...].astype(F32), axis=0) * scale[...]
    old = stream[pl.ds(x * NY, NY)].reshape(N, N)
    out[...] = 0.5 * old + 0.5 * branch


def shift(v, k):
    return lax.ppermute(v, "x", [(i, (i + k) % NX) for i in range(NX)])


def other_core(v):
    return lax.ppermute(v, "c", [(0, 1), (1, 0)])


def around(pieces):
    return [pieces[0]] + [shift(pieces[k], k) for k in range(1, NX)]


def swap(v, axis):
    return lax.all_to_all(v, axis, 0, 0, tiled=True)


def scale_rows(gate_scale, up_scale, x):
    rows = []
    for scale in (gate_scale, up_scale):
        own = lax.dynamic_slice_in_dim(scale, x * CHUNK, CHUNK, 0).reshape(2, HALF)
        rows.append(jnp.pad(own, ((0, 0), (0, PAD - HALF))))
    return jnp.concatenate(rows, axis=1)


def local(
    tokens,
    first_gain,
    first_gate,
    first_gate_scale,
    first_up,
    first_up_scale,
    first_down,
    first_down_scale,
    second_gain,
    second_gate,
    second_gate_scale,
    second_up,
    second_up_scale,
    second_down,
    second_down_scale,
):
    x = lax.axis_index("x")
    at = jnp.stack([x, lax.axis_index("y"), lax.axis_index("c")]).astype(jnp.int32)
    chunks = pltpu.VMEM((2 * NX, N, WIDE), BF)
    payload = shape(NZ, 2, N // NZ, WIDE)
    spread = shape(NZ, 2, N // NZ, PAD)

    *packed, other = call(
        pack_first_body, [shape(N, WIDE + N)] * NX + [shape(N, WIDE)], 4, [chunks], "pack_first"
    )(at, first_gate, first_up, tokens, first_gain[None])
    mine = around(packed)
    theirs = [other] + [other_core(v) for v in mine[1:]]
    sums = call(enter_first_body, payload, 8, name="enter_first")(at, *mine, *theirs)
    sums, first_down, second_gate, second_up, second_down = lax.optimization_barrier(
        (sums, first_down, second_gate, second_up, second_down)
    )
    got = swap(sums, "z")
    downs = around(
        call(pack_down_body, [shape(2 * PAD, N)] * NX, 2, name="pack_down")(
            at, first_down, second_gain[None]
        )
    )
    ups = around(
        call(pack_second_body, [shape(N, 2 * WIDE)] * NX, 2, [chunks], "pack_second")(
            at, second_gate, second_up
        )
    )
    last_downs = around(
        call(pack_down_body, [shape(2 * PAD, N)] * NX, 2, name="pack_last")(
            at, second_down, second_gain[None]
        )
    )
    hidden = call(hidden_body, spread, 2, name="hidden_first")(
        at, got, scale_rows(first_gate_scale, first_up_scale, x)
    )
    hidden = swap(hidden, "z")
    part = call(leave_first_body, shape(NX * NY, N // NY, N), 5, name="leave_first")(
        at, hidden, *downs
    )
    got = swap(part, XY)
    stream = call(stream_body, shape(NX * NY, N // NY, N, dtype=F32), 3, name="stream")(
        at, got, tokens, first_down_scale[None]
    )
    stream = swap(stream, XY)

    sums = call(enter_second_body, payload, 9, name="enter_second")(at, stream, *downs, *ups)
    got = swap(sums, "z")
    hidden = call(hidden_body, spread, 2, name="hidden_second")(
        at, got, scale_rows(second_gate_scale, second_up_scale, x)
    )
    hidden = swap(hidden, "z")
    part = call(leave_second_body, shape(NX * NY, N, N), 5, name="leave_second")(
        at, hidden, *last_downs
    )
    got = swap(part, XY)
    return call(final_body, shape(N, N, dtype=F32), 3, name="final")(
        at, got, stream, second_down_scale[None]
    )


def solution(mesh):
    torus = Mesh(
        mesh.devices.reshape(NZ, NX, mesh.shape["cb"], mesh.shape["dp"]), ("z", "x", "y", "c")
    )
    ra = ("z", "x")
    wide, tall = P(ra, "y"), P("y", ra)
    half = (P(ra), wide, P("y"), wide, P("y"), tall, P(ra))
    in_specs = (P("c", ra), *half, *half)
    return jax.shard_map(
        local, mesh=torus, in_specs=in_specs, out_specs=P("c", ra), check_vma=False
    )
```

```python
import jax
import jax.numpy as jnp
from jax import lax
from jax.experimental import pallas as pl
from jax.experimental.pallas import tpu as pltpu
from jax.sharding import Mesh
from jax.sharding import PartitionSpec as P


BF = jnp.bfloat16
F32 = jnp.float32
XY = ("x", "y")
NX, NY, NZ = 4, 4, 8
N = 128
HALF = 352
PAD = 384
WIDE = 2 * PAD
CHUNK = 2 * HALF
WIDTH = 4096
LIMIT = 16 * 2**20

SMEM = pl.BlockSpec(memory_space=pltpu.SMEM)
VMEM = pl.BlockSpec(memory_space=pltpu.VMEM)


def shape(*dims, dtype=BF):
    return jax.ShapeDtypeStruct(dims, dtype)


def call(body, outs, n_in, scratch=()):
    many = isinstance(outs, (list, tuple))
    return pl.pallas_call(
        body,
        out_shape=outs,
        in_specs=[SMEM] + [VMEM] * n_in,
        out_specs=[VMEM] * len(outs) if many else VMEM,
        scratch_shapes=list(scratch),
        compiler_params=pltpu.CompilerParams(vmem_limit_bytes=LIMIT),
    )


def high_low(v):
    high = v.astype(BF).astype(F32)
    return high, (v - high).astype(BF).astype(F32)


def padded_chunk(ref, i):
    part = ref[:, i * HALF : (i + 1) * HALF]
    return jnp.concatenate([part, jnp.zeros((N, PAD - HALF), F32)], axis=1)


def with_columns(tile, first, second):
    lane = lax.broadcasted_iota(jnp.int32, tile.shape, 1)
    at = HALF - (PAD - N)
    return jnp.where(lane == at, first, jnp.where(lane == at + 1, second, tile))


def pack_first_body(at, gate, up, tokens, gain, p0, p1, p2, p3, other, chunks):
    x, c = at[0], at[2]
    for i in range(2 * NX):
        chunks[i, :, :PAD] = padded_chunk(gate, i).astype(BF)
        chunks[i, :, PAD:] = padded_chunk(up, i).astype(BF)
    stream = tokens[...].astype(F32)
    scaled = (stream * gain[...]).astype(BF)
    high, low = high_low(jnp.sum(stream * stream, axis=1, keepdims=True))
    for k, out in enumerate((p0, p1, p2, p3)):
        index = 2 * lax.rem(x + k, NX) + c
        out[:, :WIDE] = chunks[index]
        out[:, WIDE:] = scaled
        tile = chunks[index, :, PAD - N : PAD].astype(F32)
        out[:, PAD - N : PAD] = with_columns(tile, high, low).astype(BF)
    other[...] = chunks[2 * x + 1 - c]


def pack_second_body(at, gate, up, p0, p1, p2, p3, chunks):
    x = at[0]
    for i in range(2 * NX):
        chunks[i, :, :PAD] = padded_chunk(gate, i).astype(BF)
        chunks[i, :, PAD:] = padded_chunk(up, i).astype(BF)
    for k, out in enumerate((p0, p1, p2, p3)):
        index = 2 * lax.rem(x + k, NX)
        out[:, :WIDE] = chunks[index]
        out[:, WIDE:] = chunks[index + 1]


def pack_down_body(at, down, gain, p0, p1, p2, p3):
    x = at[0]
    value = gain[...]
    high = value.astype(BF).astype(F32)
    rest = value - high
    middle = rest.astype(BF).astype(F32)
    low = rest - middle
    row = lax.broadcasted_iota(jnp.int32, (PAD - HALF, N), 0)
    tail = jnp.where(row == 0, high, jnp.where(row == 1, middle, jnp.where(row == 2, low, 0.0)))
    tail = tail.astype(BF)
    for k, out in enumerate((p0, p1, p2, p3)):
        base = lax.rem(x + k, NX) * CHUNK
        for h in range(2):
            start = pl.multiple_of(base + h * HALF, 32)
            out[h * PAD : h * PAD + HALF, :] = down[pl.ds(start, HALF), :].astype(BF)
            out[h * PAD + HALF : (h + 1) * PAD, :] = tail


def store_payload(out, slot, sums, high, low):
    tile = with_columns(sums[:, PAD - N : PAD], high, low)
    sums = jnp.concatenate([sums[:, : PAD - N], tile, sums[:, PAD:]], axis=1)
    out[:, slot] = sums.astype(BF).reshape(NZ, N // NZ, WIDE)


def dot(a, b):
    return jnp.dot(a, b, preferred_element_type=F32)


def enter_first_body(at, r0, r1, r2, r3, q0, s1, s2, s3, out):
    c = at[2]
    mine = (r0, r1, r2, r3)
    theirs = (q0, s1, s2, s3)
    scaled = jnp.concatenate([r[:, WIDE:] for r in mine], axis=1)
    squares = jnp.zeros((N, N), F32)
    for r in mine:
        squares = squares + r[:, PAD - N : PAD].astype(F32)
    lane = lax.broadcasted_iota(jnp.int32, (N, N), 1)
    at_lane = HALF - (PAD - N)
    keep = (lane == at_lane) | (lane == at_lane + 1)
    squares = jnp.sum(jnp.where(keep, squares, 0.0), axis=1, keepdims=True)
    high, low = high_low(squares)
    for slot, group in ((c, mine), (1 - c, theirs)):
        weights = jnp.concatenate([r[:, :WIDE] for r in group], axis=0)
        store_payload(out, slot, dot(scaled, weights), high, low)


def enter_second_body(at, stream, d0, d1, d2, d3, w0, w1, w2, w3, out):
    x = at[0]
    scaled = []
    squares = jnp.zeros((N, 1), F32)
    for k, d in enumerate((d0, d1, d2, d3)):
        index = lax.rem(x + NX - k, NX)
        s = stream[pl.ds(index * NY, NY)].reshape(N, N)
        squares = squares + jnp.sum(s * s, axis=1, keepdims=True)
        tail = d[HALF:PAD, :].astype(F32)
        gain = tail[0:1] + tail[1:2] + tail[2:3]
        scaled.append((s * gain).astype(BF))
    scaled = jnp.concatenate(scaled, axis=1)
    high, low = high_low(squares)
    for slot in range(2):
        cols = slice(slot * WIDE, (slot + 1) * WIDE)
        weights = jnp.concatenate([w[:, cols] for w in (w0, w1, w2, w3)], axis=0)
        store_payload(out, slot, dot(scaled, weights), high, low)


def hidden_body(at, got, scales, out):
    rows = N // NZ
    tile = jnp.zeros((rows, N), F32)
    for z in range(NZ):
        tile = tile + got[z, 0, :, PAD - N : PAD].astype(F32)
    lane = lax.broadcasted_iota(jnp.int32, (rows, N), 1)
    at_lane = HALF - (PAD - N)
    keep = (lane == at_lane) | (lane == at_lane + 1)
    total = jnp.sum(jnp.where(keep, tile, 0.0), axis=1, keepdims=True)
    inverse = lax.rsqrt(total / WIDTH + 1e-06)
    for h in range(2):
        sums = got[0, h].astype(F32)
        for z in range(1, NZ):
            sums = sums + got[z, h].astype(F32)
        scaled = sums * inverse * scales[h : h + 1, :]
        gate = scaled[:, :PAD]
        hidden = gate / (1.0 + jnp.exp(-gate)) * scaled[:, PAD:]
        hidden = hidden.astype(BF)
        for z in range(NZ):
            out[z, h] = hidden


def down_sums(hidden, pieces):
    wide = jnp.concatenate([hidden[:, h].reshape(N, PAD) for h in range(2)], axis=1)
    return [dot(wide, d[...]).astype(BF) for d in pieces]


def leave_first_body(at, hidden, d0, d1, d2, d3, out):
    x = at[0]
    for k, part in enumerate(down_sums(hidden, (d0, d1, d2, d3))):
        index = lax.rem(x + NX - k, NX)
        out[pl.ds(index * NY, NY)] = part.reshape(NY, N // NY, N)


def leave_second_body(at, hidden, d0, d1, d2, d3, out):
    x = at[0]
    for k, part in enumerate(down_sums(hidden, (d0, d1, d2, d3))):
        index = lax.rem(x + NX - k, NX)
        for y in range(NY):
            out[index * NY + y] = part


def stream_body(at, got, tokens, scale, out):
    y = at[1]
    rows = N // NY
    branch = jnp.sum(got[...].astype(F32), axis=0) * scale[...]
    old = tokens[pl.ds(pl.multiple_of(y * rows, rows), rows), :].astype(F32)
    new = 0.5 * old + 0.5 * branch
    out[...] = jnp.broadcast_to(new[None], out.shape)


def final_body(at, got, stream, scale, out):
    x = at[0]
    branch = jnp.sum(got[...].astype(F32), axis=0) * scale[...]
    old = stream[pl.ds(x * NY, NY)].reshape(N, N)
    out[...] = 0.5 * old + 0.5 * branch


def shift(v, k):
    return lax.ppermute(v, "x", [(i, (i + k) % NX) for i in range(NX)])


def other_core(v):
    return lax.ppermute(v, "c", [(0, 1), (1, 0)])


def around(pieces):
    return [pieces[0]] + [shift(pieces[k], k) for k in range(1, NX)]


def swap(v, axis):
    return lax.all_to_all(v, axis, 0, 0, tiled=True)


def scale_rows(gate_scale, up_scale, x):
    rows = []
    for scale in (gate_scale, up_scale):
        own = lax.dynamic_slice_in_dim(scale, x * CHUNK, CHUNK, 0).reshape(2, HALF)
        rows.append(jnp.pad(own, ((0, 0), (0, PAD - HALF))))
    return jnp.concatenate(rows, axis=1)


def local(
    tokens,
    first_gain,
    first_gate,
    first_gate_scale,
    first_up,
    first_up_scale,
    first_down,
    first_down_scale,
    second_gain,
    second_gate,
    second_gate_scale,
    second_up,
    second_up_scale,
    second_down,
    second_down_scale,
):
    x = lax.axis_index("x")
    at = jnp.stack([x, lax.axis_index("y"), lax.axis_index("c")]).astype(jnp.int32)
    chunks = pltpu.VMEM((2 * NX, N, WIDE), BF)
    payload = shape(NZ, 2, N // NZ, WIDE)
    spread = shape(NZ, 2, N // NZ, PAD)

    *packed, other = call(
        pack_first_body, [shape(N, WIDE + N)] * NX + [shape(N, WIDE)], 4, [chunks]
    )(at, first_gate, first_up, tokens, first_gain[None])
    mine = around(packed)
    theirs = [other] + [other_core(v) for v in mine[1:]]
    sums = call(enter_first_body, payload, 8)(at, *mine, *theirs)
    sums, first_down, second_gate, second_up, second_down = lax.optimization_barrier(
        (sums, first_down, second_gate, second_up, second_down)
    )
    got = swap(sums, "z")
    downs = around(
        call(pack_down_body, [shape(2 * PAD, N)] * NX, 2)(
            at, first_down, second_gain[None]
        ),
    )
    ups = around(
        call(pack_second_body, [shape(N, 2 * WIDE)] * NX, 2, [chunks])(
            at, second_gate, second_up
        ),
    )
    last_downs = around(
        call(pack_down_body, [shape(2 * PAD, N)] * NX, 2)(
            at, second_down, second_gain[None]
        ),
    )
    hidden = call(hidden_body, spread, 2)(
        at, got, scale_rows(first_gate_scale, first_up_scale, x)
    )
    hidden = swap(hidden, "z")
    part = call(leave_first_body, shape(NX * NY, N // NY, N), 5)(at, hidden, *downs)
    got = swap(part, XY)
    stream = call(stream_body, shape(NX * NY, N // NY, N, dtype=F32), 3)(
        at, got, tokens, first_down_scale[None]
    )
    stream = swap(stream, XY)

    sums = call(enter_second_body, payload, 9)(at, stream, *downs, *ups)
    got = swap(sums, "z")
    hidden = call(hidden_body, spread, 2)(
        at, got, scale_rows(second_gate_scale, second_up_scale, x)
    )
    hidden = swap(hidden, "z")
    part = call(leave_second_body, shape(NX * NY, N, N), 5)(at, hidden, *last_downs)
    got = swap(part, XY)
    return call(final_body, shape(N, N, dtype=F32), 3)(
        at, got, stream, second_down_scale[None]
    )


def solution(mesh):
    torus = Mesh(
        mesh.devices.reshape(NZ, NX, mesh.shape["cb"], mesh.shape["dp"]), ("z", "x", "y", "c")
    )
    ra = ("z", "x")
    wide, tall = P(ra, "y"), P("y", ra)
    half = (P(ra), wide, P("y"), wide, P("y"), tall, P(ra))
    in_specs = (P("c", ra), *half, *half)
    return jax.shard_map(
        local, mesh=torus, in_specs=in_specs, out_specs=P("c", ra), check_vma=False
    )
```

```python
import jax
import jax.numpy as jnp
from jax import lax
from jax.experimental import pallas as pl
from jax.experimental.pallas import tpu as pltpu
from jax.sharding import Mesh
from jax.sharding import PartitionSpec as P


BF = jnp.bfloat16
F32 = jnp.float32
XY = ("x", "y")
NX, NY, NZ = 4, 4, 8
N = 128
HALF = 352
PAD = 384
WIDE = 2 * PAD
CHUNK = 2 * HALF
WIDTH = 4096
LIMIT = 8 * 2**20

SMEM = pl.BlockSpec(memory_space=pltpu.SMEM)
VMEM = pl.BlockSpec(memory_space=pltpu.VMEM)
HBM = pl.BlockSpec(memory_space=pltpu.HBM)
BLOCKS = 4


def shape(*dims, dtype=BF):
    return jax.ShapeDtypeStruct(dims, dtype)


def call(body, outs, n_in, scratch=(), far=0):
    many = isinstance(outs, (list, tuple))
    kernel = pl.pallas_call(
        body,
        out_shape=outs,
        in_specs=[SMEM] + [HBM] * far + [VMEM] * (n_in - far),
        out_specs=[VMEM] * len(outs) if many else VMEM,
        scratch_shapes=list(scratch),
        compiler_params=pltpu.CompilerParams(vmem_limit_bytes=LIMIT),
    )

    def run(*args):
        there = [pltpu.with_memory_space_constraint(v, pltpu.HBM) for v in args[1 : 1 + far]]
        return kernel(args[0], *there, *args[1 + far :])

    return run


def high_low(v):
    high = v.astype(BF).astype(F32)
    return high, (v - high).astype(BF).astype(F32)


def loads(pairs, sems):
    copies = []
    for block in range(BLOCKS):
        for j, (source, target) in enumerate(pairs):
            rows = source.shape[0] // BLOCKS
            part = pl.ds(block * rows, rows)
            copies.append(
                pltpu.make_async_copy(source.at[part], target.at[part], sems.at[block, j])
            )
    for copy in copies:
        copy.start()
    return [copies[i : i + len(pairs)] for i in range(0, len(copies), len(pairs))]


def cut_chunks(gate, up, gate_here, up_here, sems, chunks):
    rows = N // BLOCKS
    for block, copies in enumerate(loads(((gate, gate_here), (up, up_here)), sems)):
        for copy in copies:
            copy.wait()
        part = slice(block * rows, (block + 1) * rows)
        for here, first in ((gate_here, 0), (up_here, PAD)):
            for i in range(2 * NX):
                cut = here[part, i * HALF : (i + 1) * HALF]
                cut = jnp.concatenate([cut, jnp.zeros((rows, PAD - HALF), F32)], axis=1)
                chunks[i, part, first : first + PAD] = cut.astype(BF)


def with_columns(tile, first, second):
    lane = lax.broadcasted_iota(jnp.int32, tile.shape, 1)
    at = HALF - (PAD - N)
    return jnp.where(lane == at, first, jnp.where(lane == at + 1, second, tile))


def pack_first_body(
    at, gate, up, tokens, gain, p0, p1, p2, p3, other, chunks, gate_here, up_here, sems, here, sem
):
    x, c = at[0], at[2]
    copy = pltpu.make_async_copy(tokens, here, sem)
    copy.start()
    cut_chunks(gate, up, gate_here, up_here, sems, chunks)
    copy.wait()
    stream = here[...].astype(F32)
    scaled = (stream * gain[...]).astype(BF)
    high, low = high_low(jnp.sum(stream * stream, axis=1, keepdims=True))
    for k, out in enumerate((p0, p1, p2, p3)):
        index = 2 * lax.rem(x + k, NX) + c
        out[:, :WIDE] = chunks[index]
        out[:, WIDE:] = scaled
        tile = chunks[index, :, PAD - N : PAD].astype(F32)
        out[:, PAD - N : PAD] = with_columns(tile, high, low).astype(BF)
    other[...] = chunks[2 * x + 1 - c]


def pack_second_body(at, gate, up, p0, p1, p2, p3, chunks, gate_here, up_here, sems):
    x = at[0]
    cut_chunks(gate, up, gate_here, up_here, sems, chunks)
    for k, out in enumerate((p0, p1, p2, p3)):
        index = 2 * lax.rem(x + k, NX)
        out[:, :WIDE] = chunks[index]
        out[:, WIDE:] = chunks[index + 1]


def pack_down_body(at, far, gain, p0, p1, p2, p3, down, sems):
    x = at[0]
    waits = loads(((far, down),), sems)
    value = gain[...]
    high = value.astype(BF).astype(F32)
    rest = value - high
    middle = rest.astype(BF).astype(F32)
    low = rest - middle
    row = lax.broadcasted_iota(jnp.int32, (PAD - HALF, N), 0)
    tail = jnp.where(row == 0, high, jnp.where(row == 1, middle, jnp.where(row == 2, low, 0.0)))
    tail = tail.astype(BF)
    for copies in waits:
        copies[0].wait()
    for k, out in enumerate((p0, p1, p2, p3)):
        base = lax.rem(x + k, NX) * CHUNK
        for h in range(2):
            start = pl.multiple_of(base + h * HALF, 32)
            out[h * PAD : h * PAD + HALF, :] = down[pl.ds(start, HALF), :].astype(BF)
            out[h * PAD + HALF : (h + 1) * PAD, :] = tail


def store_payload(out, slot, sums, high, low):
    tile = with_columns(sums[:, PAD - N : PAD], high, low)
    sums = jnp.concatenate([sums[:, : PAD - N], tile, sums[:, PAD:]], axis=1)
    out[:, slot] = sums.astype(BF).reshape(NZ, N // NZ, WIDE)


def dot(a, b):
    return jnp.dot(a, b, preferred_element_type=F32)


def enter_first_body(at, r0, r1, r2, r3, q0, s1, s2, s3, out):
    c = at[2]
    mine = (r0, r1, r2, r3)
    theirs = (q0, s1, s2, s3)
    scaled = jnp.concatenate([r[:, WIDE:] for r in mine], axis=1)
    squares = jnp.zeros((N, N), F32)
    for r in mine:
        squares = squares + r[:, PAD - N : PAD].astype(F32)
    lane = lax.broadcasted_iota(jnp.int32, (N, N), 1)
    at_lane = HALF - (PAD - N)
    keep = (lane == at_lane) | (lane == at_lane + 1)
    squares = jnp.sum(jnp.where(keep, squares, 0.0), axis=1, keepdims=True)
    high, low = high_low(squares)
    for slot, group in ((c, mine), (1 - c, theirs)):
        weights = jnp.concatenate([r[:, :WIDE] for r in group], axis=0)
        store_payload(out, slot, dot(scaled, weights), high, low)


def enter_second_body(at, stream, d0, d1, d2, d3, w0, w1, w2, w3, out):
    x = at[0]
    scaled = []
    squares = jnp.zeros((N, 1), F32)
    for k, d in enumerate((d0, d1, d2, d3)):
        index = lax.rem(x + NX - k, NX)
        s = stream[pl.ds(index * NY, NY)].reshape(N, N)
        squares = squares + jnp.sum(s * s, axis=1, keepdims=True)
        tail = d[HALF:PAD, :].astype(F32)
        gain = tail[0:1] + tail[1:2] + tail[2:3]
        scaled.append((s * gain).astype(BF))
    scaled = jnp.concatenate(scaled, axis=1)
    high, low = high_low(squares)
    for slot in range(2):
        cols = slice(slot * WIDE, (slot + 1) * WIDE)
        weights = jnp.concatenate([w[:, cols] for w in (w0, w1, w2, w3)], axis=0)
        store_payload(out, slot, dot(scaled, weights), high, low)


def hidden_body(at, got, scales, out):
    rows = N // NZ
    tile = jnp.zeros((rows, N), F32)
    for z in range(NZ):
        tile = tile + got[z, 0, :, PAD - N : PAD].astype(F32)
    lane = lax.broadcasted_iota(jnp.int32, (rows, N), 1)
    at_lane = HALF - (PAD - N)
    keep = (lane == at_lane) | (lane == at_lane + 1)
    total = jnp.sum(jnp.where(keep, tile, 0.0), axis=1, keepdims=True)
    inverse = lax.rsqrt(total / WIDTH + 1e-06)
    for h in range(2):
        sums = got[0, h].astype(F32)
        for z in range(1, NZ):
            sums = sums + got[z, h].astype(F32)
        scaled = sums * inverse * scales[h : h + 1, :]
        gate = scaled[:, :PAD]
        hidden = gate / (1.0 + jnp.exp(-gate)) * scaled[:, PAD:]
        hidden = hidden.astype(BF)
        for z in range(NZ):
            out[z, h] = hidden


def down_sums(hidden, pieces):
    wide = jnp.concatenate([hidden[:, h].reshape(N, PAD) for h in range(2)], axis=1)
    return [dot(wide, d[...]).astype(BF) for d in pieces]


def leave_first_body(at, hidden, d0, d1, d2, d3, out):
    x = at[0]
    for k, part in enumerate(down_sums(hidden, (d0, d1, d2, d3))):
        index = lax.rem(x + NX - k, NX)
        out[pl.ds(index * NY, NY)] = part.reshape(NY, N // NY, N)


def leave_second_body(at, hidden, d0, d1, d2, d3, out):
    x = at[0]
    for k, part in enumerate(down_sums(hidden, (d0, d1, d2, d3))):
        index = lax.rem(x + NX - k, NX)
        for y in range(NY):
            out[index * NY + y] = part


def stream_body(at, got, tokens, scale, out):
    y = at[1]
    rows = N // NY
    branch = jnp.sum(got[...].astype(F32), axis=0) * scale[...]
    old = tokens[pl.ds(pl.multiple_of(y * rows, rows), rows), :].astype(F32)
    new = 0.5 * old + 0.5 * branch
    out[...] = jnp.broadcast_to(new[None], out.shape)


def final_body(at, got, stream, scale, out):
    x = at[0]
    branch = jnp.sum(got[...].astype(F32), axis=0) * scale[...]
    old = stream[pl.ds(x * NY, NY)].reshape(N, N)
    out[...] = 0.5 * old + 0.5 * branch


def shift(v, k):
    return lax.ppermute(v, "x", [(i, (i + k) % NX) for i in range(NX)])


def other_core(v):
    return lax.ppermute(v, "c", [(0, 1), (1, 0)])


def around(pieces):
    return [pieces[0]] + [shift(pieces[k], k) for k in range(1, NX)]


def swap(v, axis):
    return lax.all_to_all(v, axis, 0, 0, tiled=True)


def scale_rows(gate_scale, up_scale, x):
    rows = []
    for scale in (gate_scale, up_scale):
        own = lax.dynamic_slice_in_dim(scale, x * CHUNK, CHUNK, 0).reshape(2, HALF)
        rows.append(jnp.pad(own, ((0, 0), (0, PAD - HALF))))
    return jnp.concatenate(rows, axis=1)


def local(
    tokens,
    first_gain,
    first_gate,
    first_gate_scale,
    first_up,
    first_up_scale,
    first_down,
    first_down_scale,
    second_gain,
    second_gate,
    second_gate_scale,
    second_up,
    second_up_scale,
    second_down,
    second_down_scale,
):
    x = lax.axis_index("x")
    at = jnp.stack([x, lax.axis_index("y"), lax.axis_index("c")]).astype(jnp.int32)
    columns = 2 * NX * HALF
    wide_here = pltpu.VMEM((N, columns), F32)
    sems = pltpu.SemaphoreType.DMA((BLOCKS, 2))
    cutting = [pltpu.VMEM((2 * NX, N, WIDE), BF), wide_here, wide_here, sems]
    entering = [*cutting, pltpu.VMEM((N, N), BF), pltpu.SemaphoreType.DMA(())]
    lowering = [pltpu.VMEM((columns, N), F32), pltpu.SemaphoreType.DMA((BLOCKS, 1))]
    payload = shape(NZ, 2, N // NZ, WIDE)
    spread = shape(NZ, 2, N // NZ, PAD)

    *packed, other = call(
        pack_first_body, [shape(N, WIDE + N)] * NX + [shape(N, WIDE)], 4, entering, 3
    )(at, first_gate, first_up, tokens, first_gain[None])
    mine = around(packed)
    theirs = [other] + [other_core(v) for v in mine[1:]]
    sums = call(enter_first_body, payload, 8)(at, *mine, *theirs)
    got = swap(sums, "z")
    downs = around(
        call(pack_down_body, [shape(2 * PAD, N)] * NX, 2, lowering, 1)(
            at, first_down, second_gain[None]
        ),
    )
    ups = around(
        call(pack_second_body, [shape(N, 2 * WIDE)] * NX, 2, cutting, 2)(
            at, second_gate, second_up
        ),
    )
    last_downs = around(
        call(pack_down_body, [shape(2 * PAD, N)] * NX, 2, lowering, 1)(
            at, second_down, second_gain[None]
        ),
    )
    hidden = call(hidden_body, spread, 2)(at, got, scale_rows(first_gate_scale, first_up_scale, x))
    hidden = swap(hidden, "z")
    part = call(leave_first_body, shape(NX * NY, N // NY, N), 5)(at, hidden, *downs)
    got = swap(part, XY)
    stream = call(stream_body, shape(NX * NY, N // NY, N, dtype=F32), 3)(
        at, got, tokens, first_down_scale[None]
    )
    stream = swap(stream, XY)

    sums = call(enter_second_body, payload, 9)(at, stream, *downs, *ups)
    got = swap(sums, "z")
    hidden = call(hidden_body, spread, 2)(
        at, got, scale_rows(second_gate_scale, second_up_scale, x)
    )
    hidden = swap(hidden, "z")
    part = call(leave_second_body, shape(NX * NY, N, N), 5)(at, hidden, *last_downs)
    got = swap(part, XY)
    return call(final_body, shape(N, N, dtype=F32), 3)(at, got, stream, second_down_scale[None])


def solution(mesh):
    torus = Mesh(
        mesh.devices.reshape(NZ, NX, mesh.shape["cb"], mesh.shape["dp"]), ("z", "x", "y", "c")
    )
    ra = ("z", "x")
    wide, tall = P(ra, "y"), P("y", ra)
    half = (P(ra), wide, P("y"), wide, P("y"), tall, P(ra))
    in_specs = (P("c", ra), *half, *half)
    return jax.shard_map(
        local, mesh=torus, in_specs=in_specs, out_specs=P("c", ra), check_vma=False
    )
```

```python
import jax
import jax.numpy as jnp
from jax import lax
from jax.experimental import pallas as pl
from jax.experimental.pallas import tpu as pltpu
from jax.sharding import Mesh
from jax.sharding import PartitionSpec as P


BF = jnp.bfloat16
F32 = jnp.float32
XY = ("x", "y")
NX, NY, NZ = 4, 4, 8
N = 128
HALF = 352
PAD = 384
WIDE = 2 * PAD
CHUNK = 2 * HALF
WIDTH = 4096
LIMIT = 8 * 2**20

VMEM = pl.BlockSpec(memory_space=pltpu.VMEM)
HBM = pl.BlockSpec(memory_space=pltpu.HBM)
BLOCKS = 4


def shape(*dims, dtype=BF):
    return jax.ShapeDtypeStruct(dims, dtype)


def call(body, outs, n_in, scratch=(), far=0):
    many = isinstance(outs, (list, tuple))
    kernel = pl.pallas_call(
        body,
        out_shape=outs,
        in_specs=[HBM] * far + [VMEM] * (n_in - far),
        out_specs=[VMEM] * len(outs) if many else VMEM,
        scratch_shapes=list(scratch),
        compiler_params=pltpu.CompilerParams(vmem_limit_bytes=LIMIT),
    )

    def run(*args):
        there = [pltpu.with_memory_space_constraint(v, pltpu.HBM) for v in args[:far]]
        return kernel(*there, *args[far:])

    return run


def high_low(v):
    high = v.astype(BF).astype(F32)
    return high, (v - high).astype(BF).astype(F32)


def loads(pairs, sems):
    copies = []
    for block in range(BLOCKS):
        for j, (source, target) in enumerate(pairs):
            rows = source.shape[0] // BLOCKS
            part = pl.ds(block * rows, rows)
            copies.append(
                pltpu.make_async_copy(source.at[part], target.at[part], sems.at[block, j])
            )
    for copy in copies:
        copy.start()
    return [copies[i : i + len(pairs)] for i in range(0, len(copies), len(pairs))]


def cut_chunks(gate, up, gate_here, up_here, sems, chunks):
    rows = N // BLOCKS
    for block, copies in enumerate(loads(((gate, gate_here), (up, up_here)), sems)):
        for copy in copies:
            copy.wait()
        part = slice(block * rows, (block + 1) * rows)
        for here, first in ((gate_here, 0), (up_here, PAD)):
            for i in range(2 * NX):
                cut = here[part, i * HALF : (i + 1) * HALF]
                cut = jnp.concatenate([cut, jnp.zeros((rows, PAD - HALF), F32)], axis=1)
                chunks[i, part, first : first + PAD] = cut.astype(BF)


def with_columns(tile, first, second):
    lane = lax.broadcasted_iota(jnp.int32, tile.shape, 1)
    at = HALF - (PAD - N)
    return jnp.where(lane == at, first, jnp.where(lane == at + 1, second, tile))


def pack_first_body(
    gate, up, tokens, gain, p0, p1, p2, p3, other, chunks, gate_here, up_here, sems, here, own, sem
):
    x, c = lax.axis_index("x"), lax.axis_index("c")
    copies = [
        pltpu.make_async_copy(tokens, here, sem.at[0]),
        pltpu.make_async_copy(gain, own, sem.at[1]),
    ]
    for copy in copies:
        copy.start()
    cut_chunks(gate, up, gate_here, up_here, sems, chunks)
    for copy in copies:
        copy.wait()
    stream = here[...].astype(F32)
    scaled = (stream * own[...]).astype(BF)
    high, low = high_low(jnp.sum(stream * stream, axis=1, keepdims=True))
    for k, out in enumerate((p0, p1, p2, p3)):
        index = 2 * lax.rem(x + k, NX) + c
        out[:, :WIDE] = chunks[index]
        out[:, WIDE:] = scaled
        tile = chunks[index, :, PAD - N : PAD].astype(F32)
        out[:, PAD - N : PAD] = with_columns(tile, high, low).astype(BF)
    other[...] = chunks[2 * x + 1 - c]


def pack_second_body(gate, up, p0, p1, p2, p3, chunks, gate_here, up_here, sems):
    x = lax.axis_index("x")
    cut_chunks(gate, up, gate_here, up_here, sems, chunks)
    for k, out in enumerate((p0, p1, p2, p3)):
        index = 2 * lax.rem(x + k, NX)
        out[:, :WIDE] = chunks[index]
        out[:, WIDE:] = chunks[index + 1]


def pack_down_body(far, gain, p0, p1, p2, p3, down, sems):
    x = lax.axis_index("x")
    waits = loads(((far, down),), sems)
    value = gain[...]
    high = value.astype(BF).astype(F32)
    rest = value - high
    middle = rest.astype(BF).astype(F32)
    low = rest - middle
    row = lax.broadcasted_iota(jnp.int32, (PAD - HALF, N), 0)
    tail = jnp.where(row == 0, high, jnp.where(row == 1, middle, jnp.where(row == 2, low, 0.0)))
    tail = tail.astype(BF)
    for copies in waits:
        copies[0].wait()
    for k, out in enumerate((p0, p1, p2, p3)):
        base = lax.rem(x + k, NX) * CHUNK
        for h in range(2):
            start = pl.multiple_of(base + h * HALF, 32)
            out[h * PAD : h * PAD + HALF, :] = down[pl.ds(start, HALF), :].astype(BF)
            out[h * PAD + HALF : (h + 1) * PAD, :] = tail


def store_payload(out, slot, sums, high, low):
    tile = with_columns(sums[:, PAD - N : PAD], high, low)
    sums = jnp.concatenate([sums[:, : PAD - N], tile, sums[:, PAD:]], axis=1)
    out[:, slot] = sums.astype(BF).reshape(NZ, N // NZ, WIDE)


def dot(a, b):
    return jnp.dot(a, b, preferred_element_type=F32)


def enter_first_body(r0, r1, r2, r3, q0, s1, s2, s3, out):
    c = lax.axis_index("c")
    mine = (r0, r1, r2, r3)
    theirs = (q0, s1, s2, s3)
    scaled = jnp.concatenate([r[:, WIDE:] for r in mine], axis=1)
    squares = jnp.zeros((N, N), F32)
    for r in mine:
        squares = squares + r[:, PAD - N : PAD].astype(F32)
    lane = lax.broadcasted_iota(jnp.int32, (N, N), 1)
    at_lane = HALF - (PAD - N)
    keep = (lane == at_lane) | (lane == at_lane + 1)
    squares = jnp.sum(jnp.where(keep, squares, 0.0), axis=1, keepdims=True)
    high, low = high_low(squares)
    for slot, group in ((c, mine), (1 - c, theirs)):
        weights = jnp.concatenate([r[:, :WIDE] for r in group], axis=0)
        store_payload(out, slot, dot(scaled, weights), high, low)


def enter_second_body(stream, d0, d1, d2, d3, w0, w1, w2, w3, out):
    x = lax.axis_index("x")
    scaled = []
    squares = jnp.zeros((N, 1), F32)
    for k, d in enumerate((d0, d1, d2, d3)):
        index = lax.rem(x + NX - k, NX)
        s = stream[pl.ds(index * NY, NY)].reshape(N, N)
        squares = squares + jnp.sum(s * s, axis=1, keepdims=True)
        tail = d[HALF:PAD, :].astype(F32)
        gain = tail[0:1] + tail[1:2] + tail[2:3]
        scaled.append((s * gain).astype(BF))
    scaled = jnp.concatenate(scaled, axis=1)
    high, low = high_low(squares)
    for slot in range(2):
        cols = slice(slot * WIDE, (slot + 1) * WIDE)
        weights = jnp.concatenate([w[:, cols] for w in (w0, w1, w2, w3)], axis=0)
        store_payload(out, slot, dot(scaled, weights), high, low)


def hidden_body(got, gate_scales, up_scales, out):
    x = lax.axis_index("x")
    blank = jnp.zeros((1, PAD - HALF), F32)
    rows = N // NZ
    tile = jnp.zeros((rows, N), F32)
    for z in range(NZ):
        tile = tile + got[z, 0, :, PAD - N : PAD].astype(F32)
    lane = lax.broadcasted_iota(jnp.int32, (rows, N), 1)
    at_lane = HALF - (PAD - N)
    keep = (lane == at_lane) | (lane == at_lane + 1)
    total = jnp.sum(jnp.where(keep, tile, 0.0), axis=1, keepdims=True)
    inverse = lax.rsqrt(total / WIDTH + 1e-06)
    for h in range(2):
        sums = got[0, h].astype(F32)
        for z in range(1, NZ):
            sums = sums + got[z, h].astype(F32)
        index = 2 * x + h
        gate_row, up_row = gate_scales[pl.ds(index, 1), :], up_scales[pl.ds(index, 1), :]
        row = jnp.concatenate([gate_row, blank, up_row, blank], axis=1)
        scaled = sums * inverse * row
        gate = scaled[:, :PAD]
        hidden = gate / (1.0 + jnp.exp(-gate)) * scaled[:, PAD:]
        hidden = hidden.astype(BF)
        for z in range(NZ):
            out[z, h] = hidden


def down_sums(hidden, pieces):
    wide = jnp.concatenate([hidden[:, h].reshape(N, PAD) for h in range(2)], axis=1)
    return [dot(wide, d[...]).astype(BF) for d in pieces]


def leave_first_body(hidden, d0, d1, d2, d3, out):
    x = lax.axis_index("x")
    for k, part in enumerate(down_sums(hidden, (d0, d1, d2, d3))):
        index = lax.rem(x + NX - k, NX)
        out[pl.ds(index * NY, NY)] = part.reshape(NY, N // NY, N)


def leave_second_body(hidden, d0, d1, d2, d3, out):
    x = lax.axis_index("x")
    for k, part in enumerate(down_sums(hidden, (d0, d1, d2, d3))):
        index = lax.rem(x + NX - k, NX)
        for y in range(NY):
            out[index * NY + y] = part


def stream_body(got, tokens, scale, out):
    y = lax.axis_index("y")
    rows = N // NY
    branch = jnp.sum(got[...].astype(F32), axis=0) * scale[...]
    old = tokens[pl.ds(pl.multiple_of(y * rows, rows), rows), :].astype(F32)
    new = 0.5 * old + 0.5 * branch
    out[...] = jnp.broadcast_to(new[None], out.shape)


def final_body(got, stream, scale, out):
    x = lax.axis_index("x")
    branch = jnp.sum(got[...].astype(F32), axis=0) * scale[...]
    old = stream[pl.ds(x * NY, NY)].reshape(N, N)
    out[...] = 0.5 * old + 0.5 * branch


def shift(v, k):
    return lax.ppermute(v, "x", [(i, (i + k) % NX) for i in range(NX)])


def other_core(v):
    return lax.ppermute(v, "c", [(0, 1), (1, 0)])


def around(pieces):
    return [pieces[0]] + [shift(pieces[k], k) for k in range(1, NX)]


def swap(v, axis):
    return lax.all_to_all(v, axis, 0, 0, tiled=True)


def by_chunk(scale):
    return scale.reshape(2 * NX, HALF)


def local(
    tokens,
    first_gain,
    first_gate,
    first_gate_scale,
    first_up,
    first_up_scale,
    first_down,
    first_down_scale,
    second_gain,
    second_gate,
    second_gate_scale,
    second_up,
    second_up_scale,
    second_down,
    second_down_scale,
):
    columns = 2 * NX * HALF
    wide_here = pltpu.VMEM((N, columns), F32)
    sems = pltpu.SemaphoreType.DMA((BLOCKS, 2))
    cutting = [pltpu.VMEM((2 * NX, N, WIDE), BF), wide_here, wide_here, sems]
    entering = [
        *cutting,
        pltpu.VMEM((N, N), BF),
        pltpu.VMEM((1, N), F32),
        pltpu.SemaphoreType.DMA((2,)),
    ]
    lowering = [pltpu.VMEM((columns, N), F32), pltpu.SemaphoreType.DMA((BLOCKS, 1))]
    payload = shape(NZ, 2, N // NZ, WIDE)
    spread = shape(NZ, 2, N // NZ, PAD)

    *packed, other = call(
        pack_first_body, [shape(N, WIDE + N)] * NX + [shape(N, WIDE)], 4, entering, 4
    )(first_gate, first_up, tokens, first_gain[None])
    mine = around(packed)
    theirs = [other] + [other_core(v) for v in mine[1:]]
    sums = call(enter_first_body, payload, 8)(*mine, *theirs)
    got = swap(sums, "z")
    downs = around(
        call(pack_down_body, [shape(2 * PAD, N)] * NX, 2, lowering, 1)(
            first_down, second_gain[None]
        ),
    )
    ups = around(
        call(pack_second_body, [shape(N, 2 * WIDE)] * NX, 2, cutting, 2)(second_gate, second_up),
    )
    last_downs = around(
        call(pack_down_body, [shape(2 * PAD, N)] * NX, 2, lowering, 1)(
            second_down, second_gain[None]
        ),
    )
    hidden = call(hidden_body, spread, 3)(got, by_chunk(first_gate_scale), by_chunk(first_up_scale))
    hidden = swap(hidden, "z")
    part = call(leave_first_body, shape(NX * NY, N // NY, N), 5)(
        hidden, *downs
    )
    got = swap(part, XY)
    stream = call(stream_body, shape(NX * NY, N // NY, N, dtype=F32), 3)(
        got, tokens, first_down_scale[None]
    )
    stream = swap(stream, XY)

    sums = call(enter_second_body, payload, 9)(stream, *downs, *ups)
    got = swap(sums, "z")
    hidden = call(hidden_body, spread, 3)(
        got, by_chunk(second_gate_scale), by_chunk(second_up_scale)
    )
    hidden = swap(hidden, "z")
    part = call(leave_second_body, shape(NX * NY, N, N), 5)(hidden, *last_downs)
    got = swap(part, XY)
    return call(final_body, shape(N, N, dtype=F32), 3)(got, stream, second_down_scale[None])


def solution(mesh):
    torus = Mesh(
        mesh.devices.reshape(NZ, NX, mesh.shape["cb"], mesh.shape["dp"]), ("z", "x", "y", "c")
    )
    ra = ("z", "x")
    wide, tall = P(ra, "y"), P("y", ra)
    half = (P(ra), wide, P("y"), wide, P("y"), tall, P(ra))
    in_specs = (P("c", ra), *half, *half)
    return jax.shard_map(
        local, mesh=torus, in_specs=in_specs, out_specs=P("c", ra), check_vma=False
    )
```

```python
import jax
import jax.numpy as jnp
from jax import lax
from jax.experimental import pallas as pl
from jax.experimental.pallas import tpu as pltpu
from jax.sharding import Mesh
from jax.sharding import PartitionSpec as P


BF = jnp.bfloat16
F32 = jnp.float32
XY = ("x", "y")
NX, NY, NZ = 4, 4, 8
N = 128
HALF = 352
PAD = 384
WIDE = 2 * PAD
CHUNK = 2 * HALF
WIDTH = 4096
LIMIT = 8 * 2**20

VMEM = pl.BlockSpec(memory_space=pltpu.VMEM)
HBM = pl.BlockSpec(memory_space=pltpu.HBM)
BLOCKS = 4


def shape(*dims, dtype=BF):
    return jax.ShapeDtypeStruct(dims, dtype)


def call(body, outs, n_in, scratch=(), far=0):
    many = isinstance(outs, (list, tuple))
    kernel = pl.pallas_call(
        body,
        out_shape=outs,
        in_specs=[HBM] * far + [VMEM] * (n_in - far),
        out_specs=[VMEM] * len(outs) if many else VMEM,
        scratch_shapes=list(scratch),
        compiler_params=pltpu.CompilerParams(vmem_limit_bytes=LIMIT),
    )

    def run(*args):
        there = [pltpu.with_memory_space_constraint(v, pltpu.HBM) for v in args[:far]]
        return kernel(*there, *args[far:])

    return run


def high_low(v):
    high = v.astype(BF).astype(F32)
    return high, (v - high).astype(BF).astype(F32)


def loads(pairs, sems):
    copies = []
    for block in range(BLOCKS):
        for j, (source, target) in enumerate(pairs):
            rows = source.shape[0] // BLOCKS
            part = pl.ds(block * rows, rows)
            copies.append(
                pltpu.make_async_copy(source.at[part], target.at[part], sems.at[block, j])
            )
    for copy in copies:
        copy.start()
    return [copies[i : i + len(pairs)] for i in range(0, len(copies), len(pairs))]


def cut_chunks(gate, up, gate_here, up_here, sems, chunks):
    rows = N // BLOCKS
    for block, copies in enumerate(loads(((gate, gate_here), (up, up_here)), sems)):
        for copy in copies:
            copy.wait()
        part = slice(block * rows, (block + 1) * rows)
        for here, first in ((gate_here, 0), (up_here, PAD)):
            for i in range(2 * NX):
                cut = here[part, i * HALF : (i + 1) * HALF]
                cut = jnp.concatenate([cut, jnp.zeros((rows, PAD - HALF), F32)], axis=1)
                chunks[i, part, first : first + PAD] = cut.astype(BF)


def with_columns(tile, first, second):
    lane = lax.broadcasted_iota(jnp.int32, tile.shape, 1)
    at = HALF - (PAD - N)
    return jnp.where(lane == at, first, jnp.where(lane == at + 1, second, tile))


def pack_first_body(
    gate, up, tokens, gain, p0, p1, p2, p3, other, chunks, gate_here, up_here, sems, here, own, sem
):
    x, c = lax.axis_index("x"), lax.axis_index("c")
    copies = [
        pltpu.make_async_copy(tokens, here, sem.at[0]),
        pltpu.make_async_copy(gain, own, sem.at[1]),
    ]
    for copy in copies:
        copy.start()
    cut_chunks(gate, up, gate_here, up_here, sems, chunks)
    for copy in copies:
        copy.wait()
    stream = here[...].astype(F32)
    scaled = (stream * own[...]).astype(BF)
    high, low = high_low(jnp.sum(stream * stream, axis=1, keepdims=True))
    for k, out in enumerate((p0, p1, p2, p3)):
        index = 2 * lax.rem(x + k, NX) + c
        out[:, :WIDE] = chunks[index]
        out[:, WIDE:] = scaled
        tile = chunks[index, :, PAD - N : PAD].astype(F32)
        out[:, PAD - N : PAD] = with_columns(tile, high, low).astype(BF)
    other[...] = chunks[2 * x + 1 - c]


def pack_second_body(gate, up, p0, p1, p2, p3, chunks, gate_here, up_here, sems):
    x = lax.axis_index("x")
    cut_chunks(gate, up, gate_here, up_here, sems, chunks)
    for k, out in enumerate((p0, p1, p2, p3)):
        index = 2 * lax.rem(x + k, NX)
        out[:, :WIDE] = chunks[index]
        out[:, WIDE:] = chunks[index + 1]


def pack_down_body(far, gain, p0, p1, p2, p3, down, sems):
    x = lax.axis_index("x")
    waits = loads(((far, down),), sems)
    value = gain[...]
    high = value.astype(BF).astype(F32)
    rest = value - high
    middle = rest.astype(BF).astype(F32)
    low = rest - middle
    row = lax.broadcasted_iota(jnp.int32, (PAD - HALF, N), 0)
    tail = jnp.where(row == 0, high, jnp.where(row == 1, middle, jnp.where(row == 2, low, 0.0)))
    tail = tail.astype(BF)
    for copies in waits:
        copies[0].wait()
    for k, out in enumerate((p0, p1, p2, p3)):
        base = lax.rem(x + k, NX) * CHUNK
        for h in range(2):
            start = pl.multiple_of(base + h * HALF, 32)
            out[h * PAD : h * PAD + HALF, :] = down[pl.ds(start, HALF), :].astype(BF)
            out[h * PAD + HALF : (h + 1) * PAD, :] = tail


def store_payload(out, slot, sums, high, low):
    tile = with_columns(sums[:, PAD - N : PAD], high, low)
    sums = jnp.concatenate([sums[:, : PAD - N], tile, sums[:, PAD:]], axis=1)
    out[:, slot] = sums.astype(BF).reshape(NZ, N // NZ, WIDE)


def dot(a, b):
    return jnp.dot(a, b, preferred_element_type=F32)


def enter_first_body(r0, r1, r2, r3, q0, s1, s2, s3, out):
    c = lax.axis_index("c")
    mine = (r0, r1, r2, r3)
    theirs = (q0, s1, s2, s3)
    scaled = jnp.concatenate([r[:, WIDE:] for r in mine], axis=1)
    squares = jnp.zeros((N, N), F32)
    for r in mine:
        squares = squares + r[:, PAD - N : PAD].astype(F32)
    lane = lax.broadcasted_iota(jnp.int32, (N, N), 1)
    at_lane = HALF - (PAD - N)
    keep = (lane == at_lane) | (lane == at_lane + 1)
    squares = jnp.sum(jnp.where(keep, squares, 0.0), axis=1, keepdims=True)
    high, low = high_low(squares)
    for slot, group in ((c, mine), (1 - c, theirs)):
        weights = jnp.concatenate([r[:, :WIDE] for r in group], axis=0)
        store_payload(out, slot, dot(scaled, weights), high, low)


def enter_second_body(s0, s1, s2, s3, d0, d1, d2, d3, w0, w1, w2, w3, out):
    scaled = []
    squares = jnp.zeros((N, N), F32)
    for stream, d in ((s0, d0), (s1, d1), (s2, d2), (s3, d3)):
        s = stream[...]
        squares = squares + s * s
        tail = d[HALF:PAD, :].astype(F32)
        gain = tail[0:1] + tail[1:2] + tail[2:3]
        scaled.append((s * gain).astype(BF))
    squares = jnp.sum(squares, axis=1, keepdims=True)
    scaled = jnp.concatenate(scaled, axis=1)
    high, low = high_low(squares)
    for slot in range(2):
        cols = slice(slot * WIDE, (slot + 1) * WIDE)
        weights = jnp.concatenate([w[:, cols] for w in (w0, w1, w2, w3)], axis=0)
        store_payload(out, slot, dot(scaled, weights), high, low)


def hidden_body(got, gate_scales, up_scales, out):
    x = lax.axis_index("x")
    blank = jnp.zeros((1, PAD - HALF), F32)
    rows = N // NZ
    tile = jnp.zeros((rows, N), F32)
    for z in range(NZ):
        tile = tile + got[z, 0, :, PAD - N : PAD].astype(F32)
    lane = lax.broadcasted_iota(jnp.int32, (rows, N), 1)
    at_lane = HALF - (PAD - N)
    keep = (lane == at_lane) | (lane == at_lane + 1)
    total = jnp.sum(jnp.where(keep, tile, 0.0), axis=1, keepdims=True)
    inverse = lax.rsqrt(total / WIDTH + 1e-06)
    for h in range(2):
        sums = got[0, h].astype(F32)
        for z in range(1, NZ):
            sums = sums + got[z, h].astype(F32)
        index = 2 * x + h
        gate_row, up_row = gate_scales[pl.ds(index, 1), :], up_scales[pl.ds(index, 1), :]
        row = jnp.concatenate([gate_row, blank, up_row, blank], axis=1)
        scaled = sums * inverse * row
        gate = scaled[:, :PAD]
        hidden = gate / (1.0 + jnp.exp(-gate)) * scaled[:, PAD:]
        hidden = hidden.astype(BF)
        for z in range(NZ):
            out[z, h] = hidden


def down_sums(hidden, pieces):
    wide = jnp.concatenate([hidden[:, h].reshape(N, PAD) for h in range(2)], axis=1)
    return [dot(wide, d[...]).astype(BF) for d in pieces]


def leave_body(hidden, d0, d1, d2, d3, out):
    x = lax.axis_index("x")
    for k, part in enumerate(down_sums(hidden, (d0, d1, d2, d3))):
        index = lax.rem(x + NX - k, NX)
        for y in range(NY):
            out[index * NY + y] = part


def stream_body(got, old, scale, out):
    branch = jnp.sum(got[...].astype(F32), axis=0) * scale[...]
    out[...] = 0.5 * old[...].astype(F32) + 0.5 * branch


def shift(v, k):
    return lax.ppermute(v, "x", [(i, (i + k) % NX) for i in range(NX)])


def other_core(v):
    return lax.ppermute(v, "c", [(0, 1), (1, 0)])


def around(pieces):
    return [pieces[0]] + [shift(pieces[k], k) for k in range(1, NX)]


def swap(v, axis):
    return lax.all_to_all(v, axis, 0, 0, tiled=True)


def by_chunk(scale):
    return scale.reshape(2 * NX, HALF)


def local(
    tokens,
    first_gain,
    first_gate,
    first_gate_scale,
    first_up,
    first_up_scale,
    first_down,
    first_down_scale,
    second_gain,
    second_gate,
    second_gate_scale,
    second_up,
    second_up_scale,
    second_down,
    second_down_scale,
):
    columns = 2 * NX * HALF
    wide_here = pltpu.VMEM((N, columns), F32)
    sems = pltpu.SemaphoreType.DMA((BLOCKS, 2))
    cutting = [pltpu.VMEM((2 * NX, N, WIDE), BF), wide_here, wide_here, sems]
    entering = [
        *cutting,
        pltpu.VMEM((N, N), BF),
        pltpu.VMEM((1, N), F32),
        pltpu.SemaphoreType.DMA((2,)),
    ]
    lowering = [pltpu.VMEM((columns, N), F32), pltpu.SemaphoreType.DMA((BLOCKS, 1))]
    payload = shape(NZ, 2, N // NZ, WIDE)
    spread = shape(NZ, 2, N // NZ, PAD)

    *packed, other = call(
        pack_first_body, [shape(N, WIDE + N)] * NX + [shape(N, WIDE)], 4, entering, 4
    )(first_gate, first_up, tokens, first_gain[None])
    mine = around(packed)
    theirs = [other] + [other_core(v) for v in mine[1:]]
    sums = call(enter_first_body, payload, 8)(*mine, *theirs)
    got = swap(sums, "z")
    downs = around(
        call(pack_down_body, [shape(2 * PAD, N)] * NX, 2, lowering, 1)(
            first_down, second_gain[None]
        ),
    )
    ups = around(
        call(pack_second_body, [shape(N, 2 * WIDE)] * NX, 2, cutting, 2)(second_gate, second_up),
    )
    last_downs = around(
        call(pack_down_body, [shape(2 * PAD, N)] * NX, 2, lowering, 1)(
            second_down, second_gain[None]
        ),
    )
    hidden = call(hidden_body, spread, 3)(got, by_chunk(first_gate_scale), by_chunk(first_up_scale))
    hidden = swap(hidden, "z")
    part = call(leave_body, shape(NX * NY, N, N), 5)(hidden, *downs)
    got = swap(part, XY)
    stream = call(stream_body, shape(N, N, dtype=F32), 3)(got, tokens, first_down_scale[None])
    streams = around([stream] * NX)

    sums = call(enter_second_body, payload, 12)(*streams, *downs, *ups)
    got = swap(sums, "z")
    hidden = call(hidden_body, spread, 3)(
        got, by_chunk(second_gate_scale), by_chunk(second_up_scale)
    )
    hidden = swap(hidden, "z")
    part = call(leave_body, shape(NX * NY, N, N), 5)(hidden, *last_downs)
    got = swap(part, XY)
    return call(stream_body, shape(N, N, dtype=F32), 3)(got, stream, second_down_scale[None])


def solution(mesh):
    torus = Mesh(
        mesh.devices.reshape(NZ, NX, mesh.shape["cb"], mesh.shape["dp"]), ("z", "x", "y", "c")
    )
    ra = ("z", "x")
    wide, tall = P(ra, "y"), P("y", ra)
    half = (P(ra), wide, P("y"), wide, P("y"), tall, P(ra))
    in_specs = (P("c", ra), *half, *half)
    return jax.shard_map(
        local, mesh=torus, in_specs=in_specs, out_specs=P("c", ra), check_vma=False
    )
```

```python
import jax
import jax.numpy as jnp
from jax import lax
from jax.experimental import pallas as pl
from jax.experimental.pallas import tpu as pltpu
from jax.sharding import Mesh
from jax.sharding import PartitionSpec as P


BF = jnp.bfloat16
F32 = jnp.float32
XY = ("x", "y")
NX, NY, NZ = 4, 4, 8
N = 128
HALF = 352
PAD = 384
WIDE = 2 * PAD
CHUNK = 2 * HALF
WIDTH = 4096
LIMIT = 8 * 2**20

VMEM = pl.BlockSpec(memory_space=pltpu.VMEM)
HBM = pl.BlockSpec(memory_space=pltpu.HBM)
BLOCKS = 8


def shape(*dims, dtype=BF):
    return jax.ShapeDtypeStruct(dims, dtype)


def call(body, outs, n_in, scratch=(), far=0):
    many = isinstance(outs, (list, tuple))
    kernel = pl.pallas_call(
        body,
        out_shape=outs,
        in_specs=[HBM] * far + [VMEM] * (n_in - far),
        out_specs=[VMEM] * len(outs) if many else VMEM,
        scratch_shapes=list(scratch),
        compiler_params=pltpu.CompilerParams(vmem_limit_bytes=LIMIT),
    )

    def run(*args):
        there = [pltpu.with_memory_space_constraint(v, pltpu.HBM) for v in args[:far]]
        return kernel(*there, *args[far:])

    return run


def high_low(v):
    high = v.astype(BF).astype(F32)
    return high, (v - high).astype(BF).astype(F32)


def loads(pairs, sems):
    copies = []
    for block in range(BLOCKS):
        for j, (source, target) in enumerate(pairs):
            rows = source.shape[0] // BLOCKS
            part = pl.ds(block * rows, rows)
            copies.append(
                pltpu.make_async_copy(source.at[part], target.at[part], sems.at[block, j])
            )
    for copy in copies:
        copy.start()
    return [copies[i : i + len(pairs)] for i in range(0, len(copies), len(pairs))]


def cut_chunks(gate, up, gate_here, up_here, sems, chunks):
    rows = N // BLOCKS
    for block, copies in enumerate(loads(((gate, gate_here), (up, up_here)), sems)):
        for copy in copies:
            copy.wait()
        part = slice(block * rows, (block + 1) * rows)
        for here, first in ((gate_here, 0), (up_here, PAD)):
            for i in range(2 * NX):
                cut = here[part, i * HALF : (i + 1) * HALF]
                cut = jnp.concatenate([cut, jnp.zeros((rows, PAD - HALF), F32)], axis=1)
                chunks[i, part, first : first + PAD] = cut.astype(BF)


def with_columns(tile, first, second):
    lane = lax.broadcasted_iota(jnp.int32, tile.shape, 1)
    at = HALF - (PAD - N)
    return jnp.where(lane == at, first, jnp.where(lane == at + 1, second, tile))


def pack_first_body(
    gate, up, tokens, gain, p0, p1, p2, p3, other, chunks, gate_here, up_here, sems, here, own, sem
):
    x, c = lax.axis_index("x"), lax.axis_index("c")
    copies = [
        pltpu.make_async_copy(tokens, here, sem.at[0]),
        pltpu.make_async_copy(gain, own, sem.at[1]),
    ]
    for copy in copies:
        copy.start()
    cut_chunks(gate, up, gate_here, up_here, sems, chunks)
    for copy in copies:
        copy.wait()
    stream = here[...].astype(F32)
    scaled = (stream * own[...]).astype(BF)
    high, low = high_low(jnp.sum(stream * stream, axis=1, keepdims=True))
    for k, out in enumerate((p0, p1, p2, p3)):
        index = 2 * lax.rem(x + k, NX) + c
        out[:, :WIDE] = chunks[index]
        out[:, WIDE:] = scaled
        tile = chunks[index, :, PAD - N : PAD].astype(F32)
        out[:, PAD - N : PAD] = with_columns(tile, high, low).astype(BF)
    other[...] = chunks[2 * x + 1 - c]


def pack_second_body(gate, up, p0, p1, p2, p3, other, chunks, gate_here, up_here, sems):
    x, c = lax.axis_index("x"), lax.axis_index("c")
    cut_chunks(gate, up, gate_here, up_here, sems, chunks)
    for k, out in enumerate((p0, p1, p2, p3)):
        out[...] = chunks[2 * lax.rem(x + k, NX) + c]
    other[...] = chunks[2 * x + 1 - c]


def pack_down_body(far, gain, p0, p1, p2, p3, down, sems):
    x = lax.axis_index("x")
    waits = loads(((far, down),), sems)
    value = gain[...]
    high = value.astype(BF).astype(F32)
    rest = value - high
    middle = rest.astype(BF).astype(F32)
    low = rest - middle
    row = lax.broadcasted_iota(jnp.int32, (PAD - HALF, N), 0)
    tail = jnp.where(row == 0, high, jnp.where(row == 1, middle, jnp.where(row == 2, low, 0.0)))
    tail = tail.astype(BF)
    for copies in waits:
        copies[0].wait()
    for k, out in enumerate((p0, p1, p2, p3)):
        base = lax.rem(x + k, NX) * CHUNK
        for h in range(2):
            start = pl.multiple_of(base + h * HALF, 32)
            out[h * PAD : h * PAD + HALF, :] = down[pl.ds(start, HALF), :].astype(BF)
            out[h * PAD + HALF : (h + 1) * PAD, :] = tail


def store_payload(out, slot, sums, high, low):
    tile = with_columns(sums[:, PAD - N : PAD], high, low)
    sums = jnp.concatenate([sums[:, : PAD - N], tile, sums[:, PAD:]], axis=1)
    out[:, slot] = sums.astype(BF).reshape(NZ, N // NZ, WIDE)


def dot(a, b):
    return jnp.dot(a, b, preferred_element_type=F32)


def enter_first_body(r0, r1, r2, r3, q0, s1, s2, s3, out):
    c = lax.axis_index("c")
    mine = (r0, r1, r2, r3)
    theirs = (q0, s1, s2, s3)
    scaled = jnp.concatenate([r[:, WIDE:] for r in mine], axis=1)
    squares = jnp.zeros((N, N), F32)
    for r in mine:
        squares = squares + r[:, PAD - N : PAD].astype(F32)
    lane = lax.broadcasted_iota(jnp.int32, (N, N), 1)
    at_lane = HALF - (PAD - N)
    keep = (lane == at_lane) | (lane == at_lane + 1)
    squares = jnp.sum(jnp.where(keep, squares, 0.0), axis=1, keepdims=True)
    high, low = high_low(squares)
    for slot, group in ((c, mine), (1 - c, theirs)):
        weights = jnp.concatenate([r[:, :WIDE] for r in group], axis=0)
        store_payload(out, slot, dot(scaled, weights), high, low)


def enter_second_body(
    s0, s1, s2, s3, d0, d1, d2, d3, r0, r1, r2, r3, q0, q1, q2, q3, out
):
    c = lax.axis_index("c")
    squares = jnp.zeros((N, N), F32)
    for scaled, d in ((s0, d0), (s1, d1), (s2, d2), (s3, d3)):
        tail = d[HALF:PAD, :].astype(F32)
        gain = tail[0:1] + tail[1:2] + tail[2:3]
        s = scaled[...].astype(F32) * (1.0 / gain)
        squares = squares + s * s
    high, low = high_low(jnp.sum(squares, axis=1, keepdims=True))
    scaled = jnp.concatenate([v[...] for v in (s0, s1, s2, s3)], axis=1)
    for slot, group in ((c, (r0, r1, r2, r3)), (1 - c, (q0, q1, q2, q3))):
        weights = jnp.concatenate([r[...] for r in group], axis=0)
        store_payload(out, slot, dot(scaled, weights), high, low)


def hidden_body(got, gate_scales, up_scales, out):
    x = lax.axis_index("x")
    blank = jnp.zeros((1, PAD - HALF), F32)
    rows = N // NZ
    tile = jnp.zeros((rows, N), F32)
    for z in range(NZ):
        tile = tile + got[z, 0, :, PAD - N : PAD].astype(F32)
    lane = lax.broadcasted_iota(jnp.int32, (rows, N), 1)
    at_lane = HALF - (PAD - N)
    keep = (lane == at_lane) | (lane == at_lane + 1)
    total = jnp.sum(jnp.where(keep, tile, 0.0), axis=1, keepdims=True)
    inverse = lax.rsqrt(total / WIDTH + 1e-06)
    for h in range(2):
        sums = got[0, h].astype(F32)
        for z in range(1, NZ):
            sums = sums + got[z, h].astype(F32)
        index = 2 * x + h
        gate_row, up_row = gate_scales[pl.ds(index, 1), :], up_scales[pl.ds(index, 1), :]
        row = jnp.concatenate([gate_row, blank, up_row, blank], axis=1)
        scaled = sums * inverse * row
        gate = scaled[:, :PAD]
        hidden = gate / (1.0 + jnp.exp(-gate)) * scaled[:, PAD:]
        hidden = hidden.astype(BF)
        for z in range(NZ):
            out[z, h] = hidden


def down_sums(hidden, pieces):
    wide = jnp.concatenate([hidden[:, h].reshape(N, PAD) for h in range(2)], axis=1)
    return [dot(wide, d[...]).astype(BF) for d in pieces]


def leave_body(hidden, d0, d1, d2, d3, out):
    x = lax.axis_index("x")
    for k, part in enumerate(down_sums(hidden, (d0, d1, d2, d3))):
        index = lax.rem(x + NX - k, NX)
        for y in range(NY):
            out[index * NY + y] = part


def new_stream(got, old, scale):
    branch = jnp.sum(got[...].astype(F32), axis=0) * scale[...]
    return 0.5 * old[...].astype(F32) + 0.5 * branch


def stream_body(got, old, scale, gain, out, scaled):
    new = new_stream(got, old, scale)
    out[...] = new
    scaled[...] = (new * gain[...]).astype(BF)


def final_body(got, old, scale, out):
    out[...] = new_stream(got, old, scale)


def shift(v, k):
    return lax.ppermute(v, "x", [(i, (i + k) % NX) for i in range(NX)])


def other_core(v):
    return lax.ppermute(v, "c", [(0, 1), (1, 0)])


def around(pieces):
    return [pieces[0]] + [shift(pieces[k], k) for k in range(1, NX)]


def swap(v, axis):
    return lax.all_to_all(v, axis, 0, 0, tiled=True)


def by_chunk(scale):
    return scale.reshape(2 * NX, HALF)


def local(
    tokens,
    first_gain,
    first_gate,
    first_gate_scale,
    first_up,
    first_up_scale,
    first_down,
    first_down_scale,
    second_gain,
    second_gate,
    second_gate_scale,
    second_up,
    second_up_scale,
    second_down,
    second_down_scale,
):
    columns = 2 * NX * HALF
    wide_here = pltpu.VMEM((N, columns), F32)
    sems = pltpu.SemaphoreType.DMA((BLOCKS, 2))
    cutting = [pltpu.VMEM((2 * NX, N, WIDE), BF), wide_here, wide_here, sems]
    entering = [
        *cutting,
        pltpu.VMEM((N, N), BF),
        pltpu.VMEM((1, N), F32),
        pltpu.SemaphoreType.DMA((2,)),
    ]
    lowering = [pltpu.VMEM((columns, N), F32), pltpu.SemaphoreType.DMA((BLOCKS, 1))]
    payload = shape(NZ, 2, N // NZ, WIDE)
    spread = shape(NZ, 2, N // NZ, PAD)

    *packed, other = call(
        pack_first_body, [shape(N, WIDE + N)] * NX + [shape(N, WIDE)], 4, entering, 4
    )(first_gate, first_up, tokens, first_gain[None])
    mine = around(packed)
    theirs = [other] + [other_core(v) for v in mine[1:]]
    sums = call(enter_first_body, payload, 8)(*mine, *theirs)
    got = swap(sums, "z")
    downs = around(
        call(pack_down_body, [shape(2 * PAD, N)] * NX, 2, lowering, 1)(
            first_down, second_gain[None]
        ),
    )
    *packed, other = call(
        pack_second_body, [shape(N, WIDE)] * (NX + 1), 2, cutting, 2
    )(second_gate, second_up)
    ups = around(packed)
    ups = ups + [other] + [other_core(v) for v in ups[1:]]
    last_downs = around(
        call(pack_down_body, [shape(2 * PAD, N)] * NX, 2, lowering, 1)(
            second_down, second_gain[None]
        ),
    )
    hidden = call(hidden_body, spread, 3)(got, by_chunk(first_gate_scale), by_chunk(first_up_scale))
    hidden = swap(hidden, "z")
    part = call(leave_body, shape(NX * NY, N, N), 5)(hidden, *downs)
    got = swap(part, XY)
    block = shape(N, N, dtype=F32)
    stream, scaled = call(stream_body, [block, shape(N, N)], 4)(
        got, tokens, first_down_scale[None], second_gain[None]
    )
    scaled = around([scaled] * NX)

    sums = call(enter_second_body, payload, 16)(*scaled, *downs, *ups)
    got = swap(sums, "z")
    hidden = call(hidden_body, spread, 3)(
        got, by_chunk(second_gate_scale), by_chunk(second_up_scale)
    )
    hidden = swap(hidden, "z")
    part = call(leave_body, shape(NX * NY, N, N), 5)(hidden, *last_downs)
    got = swap(part, XY)
    return call(final_body, block, 3)(got, stream, second_down_scale[None])


def solution(mesh):
    torus = Mesh(
        mesh.devices.reshape(NZ, NX, mesh.shape["cb"], mesh.shape["dp"]), ("z", "x", "y", "c")
    )
    ra = ("z", "x")
    wide, tall = P(ra, "y"), P("y", ra)
    half = (P(ra), wide, P("y"), wide, P("y"), tall, P(ra))
    in_specs = (P("c", ra), *half, *half)
    return jax.shard_map(
        local, mesh=torus, in_specs=in_specs, out_specs=P("c", ra), check_vma=False
    )
```

```python
import jax
import jax.numpy as jnp
from jax import lax
from jax.experimental import pallas as pl
from jax.experimental.pallas import tpu as pltpu
from jax.sharding import Mesh
from jax.sharding import PartitionSpec as P


BF = jnp.bfloat16
F32 = jnp.float32
XY = ("x", "y")
NX, NY, NZ = 4, 4, 8
N = 128
HALF = 352
PAD = 384
WIDE = 2 * PAD
CHUNK = 2 * HALF
WIDTH = 4096
LIMIT = 8 * 2**20

VMEM = pl.BlockSpec(memory_space=pltpu.VMEM)
HBM = pl.BlockSpec(memory_space=pltpu.HBM)
BLOCKS = 4


def shape(*dims, dtype=BF):
    return jax.ShapeDtypeStruct(dims, dtype)


def call(body, outs, n_in, scratch=(), far=0):
    many = isinstance(outs, (list, tuple))
    kernel = pl.pallas_call(
        body,
        out_shape=outs,
        in_specs=[HBM] * far + [VMEM] * (n_in - far),
        out_specs=[VMEM] * len(outs) if many else VMEM,
        scratch_shapes=list(scratch),
        compiler_params=pltpu.CompilerParams(vmem_limit_bytes=LIMIT),
    )

    def run(*args):
        there = [pltpu.with_memory_space_constraint(v, pltpu.HBM) for v in args[:far]]
        return kernel(*there, *args[far:])

    return run


def high_low(v):
    high = v.astype(BF).astype(F32)
    return high, (v - high).astype(BF).astype(F32)


def loads(pairs, sems):
    copies = []
    for block in range(BLOCKS):
        for j, (source, target) in enumerate(pairs):
            rows = source.shape[0] // BLOCKS
            part = pl.ds(block * rows, rows)
            copies.append(
                pltpu.make_async_copy(source.at[part], target.at[part], sems.at[block, j])
            )
    for copy in copies:
        copy.start()
    return [copies[i : i + len(pairs)] for i in range(0, len(copies), len(pairs))]


def cut_chunks(gate, up, gate_here, up_here, sems, chunks):
    rows = N // BLOCKS
    for block, copies in enumerate(loads(((gate, gate_here), (up, up_here)), sems)):
        for copy in copies:
            copy.wait()
        part = slice(block * rows, (block + 1) * rows)
        for here, first in ((gate_here, 0), (up_here, PAD)):
            for i in range(2 * NX):
                cut = here[part, i * HALF : (i + 1) * HALF]
                cut = jnp.concatenate([cut, jnp.zeros((rows, PAD - HALF), F32)], axis=1)
                chunks[i, part, first : first + PAD] = cut.astype(BF)


def with_columns(tile, first, second):
    lane = lax.broadcasted_iota(jnp.int32, tile.shape, 1)
    at = HALF - (PAD - N)
    return jnp.where(lane == at, first, jnp.where(lane == at + 1, second, tile))


def pack_first_body(
    gate, up, tokens, gain, p0, p1, p2, p3, other, chunks, gate_here, up_here, sems, here, own, sem
):
    x, c = lax.axis_index("x"), lax.axis_index("c")
    copies = [
        pltpu.make_async_copy(tokens, here, sem.at[0]),
        pltpu.make_async_copy(gain, own, sem.at[1]),
    ]
    for copy in copies:
        copy.start()
    cut_chunks(gate, up, gate_here, up_here, sems, chunks)
    for copy in copies:
        copy.wait()
    stream = here[...].astype(F32)
    scaled = (stream * own[...]).astype(BF)
    high, low = high_low(jnp.sum(stream * stream, axis=1, keepdims=True))
    for k, out in enumerate((p0, p1, p2, p3)):
        index = 2 * lax.rem(x + k, NX) + c
        out[:, :WIDE] = chunks[index]
        out[:, WIDE:] = scaled
        tile = chunks[index, :, PAD - N : PAD].astype(F32)
        out[:, PAD - N : PAD] = with_columns(tile, high, low).astype(BF)
    other[...] = chunks[2 * x + 1 - c]


def pack_second_body(gate, up, p0, p1, p2, p3, chunks, gate_here, up_here, sems):
    x = lax.axis_index("x")
    cut_chunks(gate, up, gate_here, up_here, sems, chunks)
    for k, out in enumerate((p0, p1, p2, p3)):
        index = 2 * lax.rem(x + k, NX)
        out[:, :WIDE] = chunks[index]
        out[:, WIDE:] = chunks[index + 1]


def pack_down_body(far, gain, p0, p1, p2, p3, down, sems):
    x = lax.axis_index("x")
    waits = loads(((far, down),), sems)
    value = gain[...]
    high = value.astype(BF).astype(F32)
    rest = value - high
    middle = rest.astype(BF).astype(F32)
    low = rest - middle
    row = lax.broadcasted_iota(jnp.int32, (PAD - HALF, N), 0)
    tail = jnp.where(row == 0, high, jnp.where(row == 1, middle, jnp.where(row == 2, low, 0.0)))
    tail = tail.astype(BF)
    for copies in waits:
        copies[0].wait()
    for k, out in enumerate((p0, p1, p2, p3)):
        base = lax.rem(x + k, NX) * CHUNK
        for h in range(2):
            start = pl.multiple_of(base + h * HALF, 32)
            out[h * PAD : h * PAD + HALF, :] = down[pl.ds(start, HALF), :].astype(BF)
            out[h * PAD + HALF : (h + 1) * PAD, :] = tail


def store_payload(out, slot, sums, high, low):
    tile = with_columns(sums[:, PAD - N : PAD], high, low)
    sums = jnp.concatenate([sums[:, : PAD - N], tile, sums[:, PAD:]], axis=1)
    out[:, slot] = sums.astype(BF).reshape(NZ, N // NZ, WIDE)


def dot(a, b):
    return jnp.dot(a, b, preferred_element_type=F32)


def enter_first_body(r0, r1, r2, r3, q0, s1, s2, s3, out):
    c = lax.axis_index("c")
    mine = (r0, r1, r2, r3)
    theirs = (q0, s1, s2, s3)
    scaled = jnp.concatenate([r[:, WIDE:] for r in mine], axis=1)
    squares = jnp.zeros((N, N), F32)
    for r in mine:
        squares = squares + r[:, PAD - N : PAD].astype(F32)
    lane = lax.broadcasted_iota(jnp.int32, (N, N), 1)
    at_lane = HALF - (PAD - N)
    keep = (lane == at_lane) | (lane == at_lane + 1)
    squares = jnp.sum(jnp.where(keep, squares, 0.0), axis=1, keepdims=True)
    high, low = high_low(squares)
    for slot, group in ((c, mine), (1 - c, theirs)):
        weights = jnp.concatenate([r[:, :WIDE] for r in group], axis=0)
        store_payload(out, slot, dot(scaled, weights), high, low)


def enter_second_body(s0, s1, s2, s3, d0, d1, d2, d3, w0, w1, w2, w3, out):
    squares = jnp.zeros((N, N), F32)
    for scaled, d in ((s0, d0), (s1, d1), (s2, d2), (s3, d3)):
        tail = d[HALF:PAD, :].astype(F32)
        gain = tail[0:1] + tail[1:2] + tail[2:3]
        s = scaled[...].astype(F32) * (1.0 / gain)
        squares = squares + s * s
    high, low = high_low(jnp.sum(squares, axis=1, keepdims=True))
    scaled = jnp.concatenate([v[...] for v in (s0, s1, s2, s3)], axis=1)
    for slot in range(2):
        cols = slice(slot * WIDE, (slot + 1) * WIDE)
        weights = jnp.concatenate([w[:, cols] for w in (w0, w1, w2, w3)], axis=0)
        store_payload(out, slot, dot(scaled, weights), high, low)


def hidden_body(got, gate_scales, up_scales, out):
    x = lax.axis_index("x")
    blank = jnp.zeros((1, PAD - HALF), F32)
    rows = N // NZ
    tile = jnp.zeros((rows, N), F32)
    for z in range(NZ):
        tile = tile + got[z, 0, :, PAD - N : PAD].astype(F32)
    lane = lax.broadcasted_iota(jnp.int32, (rows, N), 1)
    at_lane = HALF - (PAD - N)
    keep = (lane == at_lane) | (lane == at_lane + 1)
    total = jnp.sum(jnp.where(keep, tile, 0.0), axis=1, keepdims=True)
    inverse = lax.rsqrt(total / WIDTH + 1e-06)
    for h in range(2):
        sums = got[0, h].astype(F32)
        for z in range(1, NZ):
            sums = sums + got[z, h].astype(F32)
        index = 2 * x + h
        gate_row, up_row = gate_scales[pl.ds(index, 1), :], up_scales[pl.ds(index, 1), :]
        row = jnp.concatenate([gate_row, blank, up_row, blank], axis=1)
        scaled = sums * inverse * row
        gate = scaled[:, :PAD]
        hidden = gate / (1.0 + jnp.exp(-gate)) * scaled[:, PAD:]
        hidden = hidden.astype(BF)
        for z in range(NZ):
            out[z, h] = hidden


def down_sums(hidden, pieces):
    wide = jnp.concatenate([hidden[:, h].reshape(N, PAD) for h in range(2)], axis=1)
    return [dot(wide, d[...]).astype(BF) for d in pieces]


def leave_body(hidden, d0, d1, d2, d3, out):
    x = lax.axis_index("x")
    for k, part in enumerate(down_sums(hidden, (d0, d1, d2, d3))):
        index = lax.rem(x + NX - k, NX)
        for y in range(NY):
            out[index * NY + y] = part


def new_stream(got, old, scale):
    branch = jnp.sum(got[...].astype(F32), axis=0) * scale[...]
    return 0.5 * old[...].astype(F32) + 0.5 * branch


def stream_body(got, old, scale, gain, out, scaled):
    new = new_stream(got, old, scale)
    out[...] = new
    scaled[...] = (new * gain[...]).astype(BF)


def final_body(got, old, scale, out):
    out[...] = new_stream(got, old, scale)


def shift(v, k):
    return lax.ppermute(v, "x", [(i, (i + k) % NX) for i in range(NX)])


def other_core(v):
    return lax.ppermute(v, "c", [(0, 1), (1, 0)])


def around(pieces):
    return [pieces[0]] + [shift(pieces[k], k) for k in range(1, NX)]


def swap(v, axis):
    return lax.all_to_all(v, axis, 0, 0, tiled=True)


def by_chunk(scale):
    return scale.reshape(2 * NX, HALF)


def local(
    tokens,
    first_gain,
    first_gate,
    first_gate_scale,
    first_up,
    first_up_scale,
    first_down,
    first_down_scale,
    second_gain,
    second_gate,
    second_gate_scale,
    second_up,
    second_up_scale,
    second_down,
    second_down_scale,
):
    columns = 2 * NX * HALF
    wide_here = pltpu.VMEM((N, columns), F32)
    sems = pltpu.SemaphoreType.DMA((BLOCKS, 2))
    cutting = [pltpu.VMEM((2 * NX, N, WIDE), BF), wide_here, wide_here, sems]
    entering = [
        *cutting,
        pltpu.VMEM((N, N), BF),
        pltpu.VMEM((1, N), F32),
        pltpu.SemaphoreType.DMA((2,)),
    ]
    lowering = [pltpu.VMEM((columns, N), F32), pltpu.SemaphoreType.DMA((BLOCKS, 1))]
    payload = shape(NZ, 2, N // NZ, WIDE)
    spread = shape(NZ, 2, N // NZ, PAD)

    *packed, other = call(
        pack_first_body, [shape(N, WIDE + N)] * NX + [shape(N, WIDE)], 4, entering, 4
    )(first_gate, first_up, tokens, first_gain[None])
    mine = around(packed)
    theirs = [other] + [other_core(v) for v in mine[1:]]
    sums = call(enter_first_body, payload, 8)(*mine, *theirs)
    got = swap(sums, "z")
    downs = around(
        call(pack_down_body, [shape(2 * PAD, N)] * NX, 2, lowering, 1)(
            first_down, second_gain[None]
        ),
    )
    ups = around(
        call(pack_second_body, [shape(N, 2 * WIDE)] * NX, 2, cutting, 2)(second_gate, second_up),
    )
    last_downs = around(
        call(pack_down_body, [shape(2 * PAD, N)] * NX, 2, lowering, 1)(
            second_down, second_gain[None]
        ),
    )
    hidden = call(hidden_body, spread, 3)(got, by_chunk(first_gate_scale), by_chunk(first_up_scale))
    hidden = swap(hidden, "z")
    part = call(leave_body, shape(NX * NY, N, N), 5)(hidden, *downs)
    got = swap(part, XY)
    block = shape(N, N, dtype=F32)
    stream, scaled = call(stream_body, [block, shape(N, N)], 4)(
        got, tokens, first_down_scale[None], second_gain[None]
    )
    scaled = around([scaled] * NX)

    sums = call(enter_second_body, payload, 12)(*scaled, *downs, *ups)
    got = swap(sums, "z")
    hidden = call(hidden_body, spread, 3)(
        got, by_chunk(second_gate_scale), by_chunk(second_up_scale)
    )
    hidden = swap(hidden, "z")
    part = call(leave_body, shape(NX * NY, N, N), 5)(hidden, *last_downs)
    got = swap(part, XY)
    return call(final_body, block, 3)(got, stream, second_down_scale[None])


def solution(mesh):
    torus = Mesh(
        mesh.devices.reshape(NZ, NX, mesh.shape["cb"], mesh.shape["dp"]), ("z", "x", "y", "c")
    )
    ra = ("z", "x")
    wide, tall = P(ra, "y"), P("y", ra)
    half = (P(ra), wide, P("y"), wide, P("y"), tall, P(ra))
    in_specs = (P("c", ra), *half, *half)
    return jax.shard_map(
        local, mesh=torus, in_specs=in_specs, out_specs=P("c", ra), check_vma=False
    )
```
